32 devices in a mesh: fs: 8 (over z, x), tp: 4 (over y, core).
Axes of the slice: x: 2, y: 2, z: 4, core: 2. Of those that a mesh axis runs over, the one named last changes fastest.
Arguments:
- resid: bfloat16 [8192, 2048], P(('fs', 'tp')), may hold values from -6 to 6
- mix_gain: float32 [2048], replicated, may hold values from 0.1 to 1.9
- in_weight: bfloat16 [2048, 2048], P('fs', 'tp'), may hold values from -0.125 to 0.125
- conv_taps: float32 [4, 2048], P(None, 'tp'), may hold values from -3 to 3
- recur_gate_w: bfloat16 [32, 64, 64], P('tp'), may hold values from -0.75 to 0.75
- input_gate_w: bfloat16 [32, 64, 64], P('tp'), may hold values from -0.75 to 0.75
- decay_rate: float32 [2048], P('tp'), may hold values from 0.0004 to 0.03
- out_weight: bfloat16 [2048, 2048], P('tp', 'fs'), may hold values from -0.25 to 0.25
- mlp_gain: float32 [2048], replicated, may hold values from 0.1 to 1.9
- up_gate_w: bfloat16 [2048, 5632], P('fs', 'tp'), may hold values from -0.125 to 0.125
- up_val_w: bfloat16 [2048, 5632], P('fs', 'tp'), may hold values from -0.125 to 0.125
- ffn_taps: float32 [3, 5632], P(None, 'tp'), may hold values from -3 to 3
- down_weight: bfloat16 [5632, 2048], P('tp', 'fs'), may hold values from -0.15625 to 0.15625
Outputs:
- result: bfloat16 [8192, 2048], P(('fs', 'tp'))
The draws below stay inside these ranges and needn't reach their ends.
All inputs are finite; a program needn't handle non-finite values.
Results may differ from the reference program's by a relative error of at most 0.028.
Values may be sent and summed in bfloat16 or wider, within the bound.
A program may use at most 64 MiB of HBM per device.

```python
import math
import jax
import jax.numpy as jnp
from jax import lax

D = 2048
RECUR = 2048
HIDDEN_SIZE = 5632
GATE_BLOCK = 64
SEQ_LEN = 128
NBLOCKS = 32
TOKENS = 8192
N_TP = 4


def block_levels(stream_key, dims, pieces, low, high):
    gain = 1.0
    for position, parts in pieces:
        heights = jax.random.uniform(jax.random.fold_in(jax.random.fold_in(stream_key, 6), position), (parts,), jnp.float32, low / len(pieces), high / len(pieces))
        gain = gain * jnp.repeat(jnp.exp(heights), dims[position] // parts).reshape((-1,) + (1,) * (len(dims) - 1 - position))
    return gain


def noise(rng, dims, spread, reach, shards=(), kind=jnp.bfloat16):
    level = block_levels(rng, dims, shards, -0.22, 0.18) if shards else 1.0
    drawn = jax.random.normal(rng, dims, jnp.float32) * spread * level
    return jnp.minimum(jnp.maximum(drawn, -reach), reach).astype(kind)


def setup_inputs(seed: int = 0) -> dict:
    splits = jax.random.split(jax.random.key(seed), 14)
    return {
        "resid": noise(splits[0], (TOKENS, D), 1.0, 6.0, ((0, 32),)),
        "mix_gain": jnp.clip(1.0 + 0.18 * jax.random.normal(splits[1], (D,), jnp.float32), 0.1, 1.9),
        "in_weight": noise(splits[2], (D, RECUR), D ** -0.5, 0.125, ((0, 8), (1, 4))),
        "conv_taps": noise(splits[3], (4, RECUR), 0.5, 3.0, ((1, 4),), jnp.float32),
        "recur_gate_w": noise(splits[4], (NBLOCKS, GATE_BLOCK, GATE_BLOCK), GATE_BLOCK ** -0.5, 0.75, ((0, 4),)),
        "input_gate_w": noise(splits[5], (NBLOCKS, GATE_BLOCK, GATE_BLOCK), GATE_BLOCK ** -0.5, 0.75, ((0, 4),)),
        "decay_rate": jnp.clip(jnp.exp(math.log(0.03) - 4.317488 * jax.random.uniform(splits[6], (RECUR,), jnp.float32) ** block_levels(splits[6], (RECUR,), ((0, 4),), -0.2, 0.2)), 0.0004, 0.03),
        "out_weight": noise(splits[7], (RECUR, D), (RECUR // 4) ** -0.5, 0.25, ((0, 4), (1, 8))),
        "mlp_gain": jnp.clip(1.0 + 0.18 * jax.random.normal(splits[8], (D,), jnp.float32), 0.1, 1.9),
        "up_gate_w": noise(splits[9], (D, HIDDEN_SIZE), D ** -0.5, 0.125, ((0, 8), (1, 4))),
        "up_val_w": noise(splits[10], (D, HIDDEN_SIZE), D ** -0.5, 0.125, ((0, 8), (1, 4))),
        "ffn_taps": noise(splits[11], (3, HIDDEN_SIZE), 0.6, 3.0, ((1, 4),), jnp.float32),
        "down_weight": noise(splits[12], (HIDDEN_SIZE, D), (HIDDEN_SIZE // 4) ** -0.5, 0.15625, ((0, 4), (1, 8))),
    }


def rms_scale(rows_in, gain_vec):
    wide = rows_in.astype(jnp.float32)
    return wide * lax.rsqrt(lax.optimization_barrier(jnp.mean(wide * wide, axis=-1, keepdims=True)) + 1e-06) * gain_vec

def causal_taps(values, tap_weights):
    width = tap_weights.shape[0]
    length = values.shape[1]
    padded = jnp.pad(values, ((0, 0), (width - 1, 0), (0, 0)))
    summed = jnp.zeros_like(values)
    for tap_index in range(width):
        summed = summed + padded[:, tap_index:tap_index + length] * tap_weights[tap_index]
    return summed

def combine(earlier, later):
    return (earlier[0] * later[0], later[0] * earlier[1] + later[1])

def group_sum(left, right, groups):
    step_size = left.shape[1] // groups
    summed = jnp.zeros((left.shape[0], right.shape[1]), jnp.float32)
    for group in range(groups):
        term = jnp.dot(left[:, group * step_size:(group + 1) * step_size], right[group * step_size:(group + 1) * step_size], preferred_element_type=jnp.float32)
        term = lax.optimization_barrier(term.astype(jnp.bfloat16))
        summed = summed + term.astype(jnp.float32)
    return summed

def reference(resid, mix_gain, in_weight, conv_taps, recur_gate_w, input_gate_w, decay_rate, out_weight, mlp_gain, up_gate_w, up_val_w, ffn_taps, down_weight):
    seqs = TOKENS // SEQ_LEN
    normed = rms_scale(resid, mix_gain).astype(jnp.bfloat16)
    projected = jnp.dot(normed, in_weight, preferred_element_type=jnp.float32).astype(jnp.bfloat16)
    conv = causal_taps(projected.astype(jnp.float32).reshape(seqs, SEQ_LEN, RECUR), conv_taps)
    blocks = conv.astype(jnp.bfloat16).astype(jnp.float32).reshape(seqs, SEQ_LEN, NBLOCKS, GATE_BLOCK)
    rgate = jax.nn.sigmoid(jnp.einsum('slnd,nde->slne', blocks, recur_gate_w.astype(jnp.float32)).reshape(seqs, SEQ_LEN, RECUR))
    igate = jax.nn.sigmoid(jnp.einsum('slnd,nde->slne', blocks, input_gate_w.astype(jnp.float32)).reshape(seqs, SEQ_LEN, RECUR))
    logdecay = -8.0 * rgate * decay_rate
    decay = jnp.exp(logdecay)
    drive = jnp.sqrt(-jnp.expm1(2.0 * logdecay)) * (igate * conv)
    state = lax.associative_scan(combine, (decay, drive), axis=1)[1]
    recurred = state.astype(jnp.bfloat16).reshape(TOKENS, RECUR)
    mixed_sum = group_sum(recurred, out_weight, N_TP)
    middle = (resid.astype(jnp.float32) + mixed_sum).astype(jnp.bfloat16)
    normed_two = rms_scale(middle, mlp_gain).astype(jnp.bfloat16)
    gate_pre = jnp.dot(normed_two, up_gate_w, preferred_element_type=jnp.float32).astype(jnp.bfloat16)
    value_pre = jnp.dot(normed_two, up_val_w, preferred_element_type=jnp.float32).astype(jnp.bfloat16)
    gate_conv = causal_taps(gate_pre.astype(jnp.float32).reshape(seqs, SEQ_LEN, HIDDEN_SIZE), ffn_taps).reshape(TOKENS, HIDDEN_SIZE)
    hidden = (jax.nn.silu(gate_conv) * value_pre.astype(jnp.float32)).astype(jnp.bfloat16)
    ffn_sum = group_sum(hidden, down_weight, N_TP)
    return (middle.astype(jnp.float32) + ffn_sum).astype(jnp.bfloat16)
```

```python
import functools

import jax
import jax.numpy as jnp
from jax import lax
from jax.experimental import pallas as pl
from jax.experimental.pallas import tpu as pltpu
from jax.sharding import PartitionSpec as P

GATE_BLOCK = 64
SEQ_LEN = 128
LANES = 128
CORES = 2


def rms_scale(rows_in, gain_vec):
    wide = rows_in.astype(jnp.float32)
    return wide * lax.rsqrt(jnp.mean(wide * wide, axis=-1, keepdims=True) + 1e-06) * gain_vec


def causal_taps(values, tap_weights):
    width = tap_weights.shape[0]
    length = values.shape[1]
    padded = jnp.pad(values, ((0, 0), (width - 1, 0), (0, 0)))
    summed = jnp.zeros_like(values)
    for tap_index in range(width):
        summed = summed + padded[:, tap_index : tap_index + length] * tap_weights[tap_index]
    return summed


def negative_expm1(arg):
    series = jnp.ones_like(arg)
    for order in range(8, 1, -1):
        series = 1.0 + arg * (1.0 / order) * series
    return jnp.where(arg > -0.5, -arg * series, 1.0 - jnp.exp(arg))


def shift_rows(values, distance, rows, fill):
    return jnp.where(rows >= distance, pltpu.roll(values, distance, 0), fill)


def recurrence_kernel(projected_ref, taps_ref, gates_ref, rate_ref, out_ref):
    width = taps_ref.shape[0]
    rows = lax.broadcasted_iota(jnp.int32, (SEQ_LEN, LANES), 0)
    for chunk in range(projected_ref.shape[1] // LANES):
        cols = slice(chunk * LANES, (chunk + 1) * LANES)
        values = projected_ref[:, cols].astype(jnp.float32)
        conv = values * taps_ref[width - 1 : width, cols]
        for back in range(1, width):
            tap = taps_ref[width - 1 - back : width - back, cols]
            conv = conv + shift_rows(values, back, rows, 0.0) * tap
        gates = jax.nn.sigmoid(
            jnp.dot(
                conv.astype(jnp.bfloat16), gates_ref[chunk], preferred_element_type=jnp.float32
            )
        )
        rgate = gates[:, :LANES]
        igate = gates[:, LANES:]
        logdecay = -8.0 * rgate * rate_ref[:, cols]
        decay = jnp.exp(logdecay)
        state = jnp.sqrt(negative_expm1(2.0 * logdecay)) * (igate * conv)
        distance = 1
        while distance < SEQ_LEN:
            state = state + decay * shift_rows(state, distance, rows, 0.0)
            if 2 * distance < SEQ_LEN:
                decay = decay * shift_rows(decay, distance, rows, 1.0)
            distance *= 2
        out_ref[:, cols] = state.astype(jnp.bfloat16)


def pair_blocks(blocks):
    pairs = blocks.reshape(-1, 2, GATE_BLOCK, GATE_BLOCK)
    blank = jnp.zeros_like(pairs[:, 0])
    upper = jnp.concatenate([pairs[:, 0], blank], axis=2)
    lower = jnp.concatenate([blank, pairs[:, 1]], axis=2)
    return jnp.concatenate([upper, lower], axis=1)


def recurrence(projected, conv_taps, gates, decay_rate):
    count, channels = projected.shape
    whole = lambda shape: pl.BlockSpec(shape, lambda seq: (0,) * len(shape))
    return pl.pallas_call(
        recurrence_kernel,
        grid=(count // SEQ_LEN,),
        in_specs=[
            pl.BlockSpec((SEQ_LEN, channels), lambda seq: (seq, 0)),
            whole(conv_taps.shape),
            whole(gates.shape),
            whole((1, channels)),
        ],
        out_specs=pl.BlockSpec((SEQ_LEN, channels), lambda seq: (seq, 0)),
        out_shape=jax.ShapeDtypeStruct(projected.shape, jnp.bfloat16),
        cost_estimate=pl.CostEstimate(
            flops=count * channels * 600, bytes_accessed=count * channels * 4,
            transcendentals=count * channels * 6,
        ),
    )(projected, conv_taps, gates, decay_rate.reshape(1, channels))


def gather_groups(block, n_tp):
    sides = n_tp // CORES
    swap = [(i, i ^ 1) for i in range(n_tp)]
    groups = []
    for distance in range(sides):
        mine = block
        if distance:
            back = [
                (i, ((i // CORES - distance) % sides) * CORES + i % CORES) for i in range(n_tp)
            ]
            mine = lax.ppermute(block, "tp", back)
        groups.append(jnp.concatenate([mine, lax.ppermute(mine, "tp", swap)], axis=0))
    return groups


def scatter_sum(partial_of, n_tp):
    sides = n_tp // CORES
    swap = [(i, i ^ 1) for i in range(n_tp)]
    total = 0.0
    for distance in reversed(range(sides)):
        partial = partial_of(distance)
        half = partial.shape[0] // 2
        other = lax.ppermute(partial[half:], "tp", swap)
        pair = partial[:half].astype(jnp.float32) + other.astype(jnp.float32)
        if distance:
            ahead = [
                (i, ((i // CORES + distance) % sides) * CORES + i % CORES) for i in range(n_tp)
            ]
            pair = lax.ppermute(pair.astype(jnp.bfloat16), "tp", ahead).astype(jnp.float32)
        total = total + pair
    return total


def gather_weight(block, n_fs, n_tp):
    inner = n_tp // CORES if n_fs % (n_tp // CORES) == 0 else 1
    outer = n_fs // inner
    me = lax.axis_index("fs")
    parts = [block]
    for distance in range(1, outer):
        back = [(i, (i - distance * inner) % n_fs) for i in range(n_fs)]
        parts.append(lax.ppermute(block, "fs", back))
    start = lax.rem(outer - me // inner, outer)
    column = lax.dynamic_slice_in_dim(jnp.stack(parts + parts[:-1]), start, outer, 0)
    parts = [column]
    for distance in range(1, inner):
        back = [(i, i // inner * inner + (i - distance) % inner) for i in range(n_fs)]
        parts.append(lax.ppermute(column, "fs", back))
    start = lax.rem(inner - lax.rem(me, inner), inner)
    stacked = jnp.stack(parts + parts[:-1], axis=1)
    stacked = lax.dynamic_slice_in_dim(stacked, start, inner, 1)
    return stacked.reshape((n_fs,) + block.shape)


def side_by_side(stacked):
    return jnp.transpose(stacked, (1, 0, 2)).reshape(stacked.shape[1], -1)


def dot(left, right):
    return jnp.dot(left, right, preferred_element_type=jnp.float32).astype(jnp.bfloat16)


def shards(
    n_fs,
    n_tp,
    resid,
    mix_gain,
    in_weight,
    conv_taps,
    recur_gate_w,
    input_gate_w,
    decay_rate,
    out_weight,
    mlp_gain,
    up_gate_w,
    up_val_w,
    ffn_taps,
    down_weight,
):
    gate_full = lax.all_gather(up_gate_w, "fs", axis=0, tiled=True)
    val_full = lax.all_gather(up_val_w, "fs", axis=0, tiled=True)
    cut = down_weight.shape[0] - down_weight.shape[0] // (2 * LANES) * LANES
    down_head = lax.all_gather(down_weight[:cut], "fs", axis=1, tiled=True)
    in_full = gather_weight(in_weight, n_fs, n_tp).reshape(-1, in_weight.shape[1])
    out_full = side_by_side(gather_weight(out_weight, n_fs, n_tp))
    later = lax.optimization_barrier((down_weight[cut:], in_full))[0]
    down_tail = side_by_side(gather_weight(later, n_fs, n_tp))
    gates = jnp.concatenate([pair_blocks(recur_gate_w), pair_blocks(input_gate_w)], axis=2)

    normed = rms_scale(resid, mix_gain).astype(jnp.bfloat16)
    recurred = [
        recurrence(dot(rows, in_full), conv_taps, gates, decay_rate)
        for rows in gather_groups(normed, n_tp)
    ]
    mixed_sum = scatter_sum(lambda distance: dot(recurred[distance], out_full), n_tp)
    middle = (resid.astype(jnp.float32) + mixed_sum).astype(jnp.bfloat16)
    normed_two = rms_scale(middle, mlp_gain).astype(jnp.bfloat16)

    hidden = []
    for rows in gather_groups(normed_two, n_tp):
        gate_pre = dot(rows, gate_full)
        value_pre = dot(rows, val_full)
        seqs = gate_pre.shape[0] // SEQ_LEN
        gate_conv = causal_taps(
            gate_pre.astype(jnp.float32).reshape(seqs, SEQ_LEN, -1), ffn_taps
        ).reshape(gate_pre.shape)
        hidden.append((jax.nn.silu(gate_conv) * value_pre.astype(jnp.float32)).astype(jnp.bfloat16))
    tails = [
        jnp.dot(rows[:, cut:], down_tail, preferred_element_type=jnp.float32) for rows in hidden
    ]

    def down_partial(distance):
        head = jnp.dot(hidden[distance][:, :cut], down_head, preferred_element_type=jnp.float32)
        return (head + tails[distance]).astype(jnp.bfloat16)

    ffn_sum = scatter_sum(down_partial, n_tp)
    return (middle.astype(jnp.float32) + ffn_sum).astype(jnp.bfloat16)


MESH = pl.DeviceIdType.MESH
SIDES = 2
VMEM_BYTES = 66_000_000


def fits(n_fs, n_tp):
    return n_tp == SIDES * CORES and n_fs % SIDES == 0 and n_fs >= 2 * SIDES


def line_order(depth, z):
    ranks = []
    for here in range(depth):
        up_first = here < depth / 2
        others = [p for p in range(depth) if p != here]
        others.sort(key=lambda p: (abs(p - here), (p < here) == up_first))
        ranks.append([here] + others)
    order = []
    for rank in range(depth):
        place = jnp.int32(0)
        for here in range(depth):
            place = jnp.where(z == here, ranks[here][rank], place)
        order.append(place)
    return order


def resident_kernel(
    depth,
    resid, gain_one, gain_two, params, gates, in_w, out_w, gate_w, val_w, down_w,
    result,
    in_full, out_full, up_full, down_full, param_full, gate_full,
    normed, proj, recurred, mix_own, mix_send, mix_recv, middle, rows_two, hidden,
    ffn_own, ffn_send, ffn_recv,
    local_sem, line_up, line_down, line_recv, side_send, side_recv, core_send, core_recv,
    swap_send, swap_recv, pair_send, pair_recv, row_sems, mix_sems_s, mix_sems_r,
    ag_send, ag_recv, rs_send, rs_recv,
):
    f32, bf16 = jnp.float32, jnp.bfloat16
    fs, tp = lax.axis_index("fs"), lax.axis_index("tp")
    z, x = fs // SIDES, lax.rem(fs, SIDES)
    y, c = tp // CORES, lax.rem(tp, CORES)
    rows, width = resid.shape
    slab = in_w.shape[0]
    chans = in_w.shape[1]
    tiles = gate_w.shape[1] // LANES
    slabs = width // slab
    n_seq = rows // SEQ_LEN
    order = line_order(depth, z)
    straight = x == c

    at = lambda zz, xx, yy, cc: (zz * SIDES + xx, yy * CORES + cc)
    up, down = at(z + 1, x, y, c), at(z - 1, x, y, c)
    side, core, swap = at(z, 1 - x, y, c), at(z, x, y, 1 - c), at(z, c, y, x)
    across, diag = at(z, x, 1 - y, c), at(z, 1 - x, 1 - y, c)
    has_up, has_down = z < depth - 1, z > 0

    flights = []

    def send(src, dst, ss, rs, dev, when=None):
        make = lambda: pltpu.make_async_remote_copy(
            src_ref=src, dst_ref=dst, send_sem=ss, recv_sem=rs, device_id=dev, device_id_type=MESH
        )
        if when is None:
            make().start()
        else:
            pl.when(when)(lambda: make().start())
        flights.append((when, make))

    def arrive(dst, rs):
        pltpu.make_async_remote_copy(
            src_ref=dst, dst_ref=dst, send_sem=rs, recv_sem=rs, device_id=core, device_id_type=MESH
        ).wait_recv()

    def row_slab(zz, xx):
        return pl.ds(pl.multiple_of((zz * SIDES + xx) * slab, slab), slab)

    def place(a, zz, xx, cc):
        if a == 0:
            return in_full.at[cc, row_slab(zz, xx), :]
        if a == 1:
            return out_full.at[zz * SIDES + xx, pl.ds(pl.multiple_of(cc * chans, chans), chans), :]
        if a == 2:
            return up_full.at[:, row_slab(zz, xx), :]
        return down_full.at[zz * SIDES + xx]

    def mine(a, zz):
        return place(a, zz, x, c) if a < 2 else place(a, zz, c, c)

    def theirs(a, zz):
        return place(a, zz, x, 1 - c) if a < 2 else place(a, zz, 1 - c, c)

    def onward(a, zz, src=None, when=None, own=False):
        dst = mine(a, zz)
        src = dst if src is None else src
        both = (lambda p: p) if when is None else (lambda p: jnp.logical_and(p, when))
        if own:
            ups, downs = has_up, has_down
        else:
            ups = jnp.logical_and(zz < z, has_up)
            downs = jnp.logical_and(zz > z, has_down)
        send(src, dst, line_up.at[a, zz], line_recv.at[a, zz], up, both(ups))
        send(src, dst, line_down.at[a, zz], line_recv.at[a, zz], down, both(downs))
        if a < 2:
            send(src, dst, side_send.at[a, zz], side_recv.at[a, zz], side)
            send(src, dst, core_send.at[a, zz, 0], core_recv.at[a, zz, x], core)
        else:
            send(src, dst, core_send.at[a, zz, 0], core_recv.at[a, zz, 0], core, when)

    def line_step(a, rank, when=None):
        zz = order[rank]
        if when is None:
            arrive(mine(a, zz), line_recv.at[a, zz])
        else:
            pl.when(when)(lambda: arrive(mine(a, zz), line_recv.at[a, zz]))
        onward(a, zz, when=when)

    def side_step(a, rank):
        zz = order[rank]
        dst = place(a, zz, 1 - x, c)
        arrive(dst, side_recv.at[a, zz])
        send(dst, dst, core_send.at[a, zz, 1], core_recv.at[a, zz, 1 - x], core)

    def own_copy(a):
        if a == 0:
            return [pltpu.make_async_copy(in_w, mine(0, z), local_sem.at[0])]
        if a == 1:
            return [pltpu.make_async_copy(out_w, mine(1, z), local_sem.at[1])]
        if a == 3:
            return [pltpu.make_async_copy(down_w, mine(3, z), local_sem.at[3])]

    def up_parts():
        for tile in range(tiles):
            for half, weight in enumerate((gate_w, val_w)):
                yield (
                    weight.at[:, pl.ds(tile * LANES, LANES)],
                    up_full.at[tile, row_slab(z, x), pl.ds(half * LANES, LANES)],
                )

    for a, weight in ((0, in_w), (1, out_w)):
        own_copy(a)[0].start()
        onward(a, z, src=weight, own=True)
    for i, (ref, full) in enumerate(((params, param_full), (gates, gate_full))):
        pltpu.make_async_copy(ref, full.at[c], local_sem.at[4 + i]).start()
        send(ref, full.at[c], pair_send.at[i], pair_recv.at[i], core)

    @pl.when(straight)
    def _():
        for src, dst in up_parts():
            pltpu.make_async_copy(src, dst, local_sem.at[2]).start()
        own_copy(3)[0].start()

    wide = resid[...].astype(f32)
    scale = lax.rsqrt(jnp.mean(wide * wide, axis=-1, keepdims=True) + 1e-06)
    normed[0:rows, :] = (wide * scale * gain_one[...]).astype(bf16)
    send(normed.at[pl.ds(0, rows), :], normed.at[pl.ds(rows, rows), :], row_sems.at[0], row_sems.at[1], across)

    for rank in range(1, depth):
        for a in (0, 1):
            line_step(a, rank)
        for a in (0, 1):
            side_step(a, rank - 1)

    @pl.when(straight)
    def _():
        pltpu.make_async_copy(mine(2, z), mine(2, z), local_sem.at[2]).wait()
        own_copy(3)[0].wait()

    @pl.when(jnp.logical_not(straight))
    def _():
        for src, dst in up_parts():
            pltpu.make_async_remote_copy(
                src_ref=src, dst_ref=dst, send_sem=swap_send.at[0], recv_sem=swap_recv.at[0],
                device_id=swap, device_id_type=MESH,
            ).start()

    crossed = jnp.logical_not(straight)
    send(down_w, place(3, z, x, c), swap_send.at[1], swap_recv.at[1], swap, crossed)
    onward(2, z, when=straight, own=True)
    for a in (0, 1):
        side_step(a, depth - 1)

    for a in (0, 1):
        own_copy(a)[0].wait()
    for i, (ref, full) in enumerate(((params, param_full), (gates, gate_full))):
        pltpu.make_async_copy(ref, full.at[c], local_sem.at[4 + i]).wait()
        arrive(full.at[1 - c], pair_recv.at[i])
    for rank in range(depth):
        zz = order[rank]
        for xx in range(SIDES):
            arrive(place(0, zz, xx, 1 - c), core_recv.at[0, zz, xx])
    arrive(normed.at[pl.ds(rows, rows), :], row_sems.at[1])

    wide_n = 2 * LANES
    per = chans // wide_n

    def project(i, _):
        cc, h = i // per, lax.rem(i, per)
        lanes = pl.ds(pl.multiple_of(h * wide_n, wide_n), wide_n)
        to = pl.ds(pl.multiple_of(i * wide_n, wide_n), wide_n)
        proj[:, to] = jnp.dot(normed[...], in_full[cc, :, lanes], preferred_element_type=f32).astype(bf16)
        return 0

    lax.fori_loop(0, CORES * per, project, 0)

    position = lax.broadcasted_iota(jnp.int32, (SEQ_LEN, LANES), 0)
    taps = params_taps = 4
    chan_tiles = chans // LANES

    def recur(seq):
        where = pl.ds(seq * SEQ_LEN, SEQ_LEN)

        def tile_step(i, _):
            cc, u = i // chan_tiles, lax.rem(i, chan_tiles)
            cols = pl.ds(pl.multiple_of(u * LANES, LANES), LANES)
            to = pl.ds(pl.multiple_of(i * LANES, LANES), LANES)
            values = proj[where, to].astype(f32)
            table = param_full[cc, :, cols]
            conv = values * table[taps - 1 : taps]
            for back in range(1, taps):
                conv = conv + shift_rows(values, back, position, 0.0) * table[taps - 1 - back : taps - back]
            both = jax.nn.sigmoid(jnp.dot(conv.astype(bf16), gate_full[cc, u], preferred_element_type=f32))
            logdecay = -8.0 * both[:, :LANES] * table[taps : taps + 1]
            decay = jnp.exp(logdecay)
            state = jnp.sqrt(negative_expm1(2.0 * logdecay)) * (both[:, LANES:] * conv)
            distance = 1
            while distance < SEQ_LEN:
                state = state + decay * shift_rows(state, distance, position, 0.0)
                if 2 * distance < SEQ_LEN:
                    decay = decay * shift_rows(decay, distance, position, 1.0)
                distance *= 2
            recurred[where, to] = state.astype(bf16)
            return 0

        lax.fori_loop(0, CORES * chan_tiles, tile_step, 0)

    half_way = n_seq
    for seq in range(2 * n_seq):
        recur(2 * n_seq - 1 - seq)
        if seq == half_way - 1 + (n_seq > 1):
            line_step(2, 1, when=straight)

    def swapped():
        arrive(mine(2, z), swap_recv.at[0])

    pl.when(crossed)(swapped)
    onward(2, z, when=crossed, own=True)

    for rank in range(depth):
        zz = order[rank]
        for xx in range(SIDES):
            arrive(place(1, zz, xx, 1 - c), core_recv.at[1, zz, xx])

    def mix_copy(j):
        return pltpu.make_async_remote_copy(
            src_ref=mix_send.at[j], dst_ref=mix_recv.at[j], send_sem=mix_sems_s.at[j],
            recv_sem=mix_sems_r.at[j], device_id=across, device_id_type=MESH,
        )

    def mix_other(j, _):
        mix_send[j] = jnp.dot(recurred[rows:, :], out_full[j], preferred_element_type=f32).astype(bf16)
        mix_copy(j).start()
        return 0

    lax.fori_loop(0, slabs, mix_other, 0)

    def mix_mine(j, _):
        mix_own[j] = jnp.dot(recurred[:rows, :], out_full[j], preferred_element_type=f32)
        return 0

    lax.fori_loop(0, slabs, mix_mine, 0)
    line_step(2, 1, when=crossed)

    total = jnp.zeros((rows, 1), f32)
    for j in range(slabs):
        mix_copy(j).wait_recv()
        lanes = slice(j * slab, (j + 1) * slab)
        value = (resid[:, lanes].astype(f32) + (mix_own[j] + mix_recv[j].astype(f32))).astype(bf16)
        middle[:, lanes] = value
        value = value.astype(f32)
        total = total + jnp.sum(value * value, axis=-1, keepdims=True)
    scale = lax.rsqrt(total * (1.0 / width) + 1e-06)
    rows_two[0:rows, :] = (middle[...].astype(f32) * scale * gain_two[...]).astype(bf16)

    part = rows // 2
    where = lambda slot, half: rows_two.at[pl.ds(slot * rows + half * part, part), :]
    send(where(0, 1), where(1, 1), ag_send.at[0, 0], ag_recv.at[0, 0], side)
    send(where(0, 0), where(2, 0), ag_send.at[1, 0], ag_recv.at[1, 0], across)
    send(where(0, 0), where(1, 0), ag_send.at[0, 1], ag_recv.at[0, 1], side)
    send(where(0, 1), where(2, 1), ag_send.at[1, 1], ag_recv.at[1, 1], across)
    line_step(2, 2)
    arrive(where(1, 1), ag_recv.at[0, 0])
    send(where(1, 1), where(3, 1), ag_send.at[1, 2], ag_recv.at[1, 2], across)
    arrive(where(2, 0), ag_recv.at[1, 0])
    send(where(2, 0), where(3, 0), ag_send.at[0, 2], ag_recv.at[0, 2], side)
    for rank in range(3, depth):
        line_step(2, rank)
    pl.when(crossed)(lambda: arrive(mine(3, z), swap_recv.at[1]))
    onward(3, z, own=True)

    arrive(where(1, 0), ag_recv.at[0, 1])
    arrive(where(2, 1), ag_recv.at[1, 1])
    arrive(where(3, 0), ag_recv.at[0, 2])
    arrive(where(3, 1), ag_recv.at[1, 2])
    for rank in range(depth):
        arrive(theirs(2, order[rank]), core_recv.at[2, order[rank], 0])

    lift = 2 * rows
    row_in_seq = lax.rem(lax.broadcasted_iota(jnp.int32, (lift, LANES), 0), SEQ_LEN)

    def raise_tile(t, _):
        cols = pl.ds(pl.multiple_of(t * LANES, LANES), LANES)
        table = param_full[x, :, pl.ds(pl.multiple_of(chans + t * LANES, LANES), LANES)]
        for block in range(2):
            here = slice(block * lift, (block + 1) * lift)
            pre = jnp.dot(rows_two[here, :], up_full[t], preferred_element_type=f32)
            gate = pre[:, :LANES].astype(bf16).astype(f32)
            value = pre[:, LANES:].astype(bf16).astype(f32)
            conv = gate * table[2:3]
            for back in (1, 2):
                conv = conv + shift_rows(gate, back, row_in_seq, 0.0) * table[2 - back : 3 - back]
            hidden[here, cols] = (jax.nn.silu(conv) * value).astype(bf16)
        return 0

    first = tiles // 2
    lax.fori_loop(0, first, raise_tile, 0)
    line_step(3, 1)
    lax.fori_loop(first, tiles, raise_tile, 0)

    def rs_copy(peer, j):
        return pltpu.make_async_remote_copy(
            src_ref=ffn_send.at[peer, j], dst_ref=ffn_recv.at[peer, j], send_sem=rs_send.at[peer, j],
            recv_sem=rs_recv.at[peer, j], device_id=(side, across, diag)[peer], device_id_type=MESH,
        )

    for rank in range(depth):
        zz = order[rank]
        if rank >= 2:
            line_step(3, rank)
        arrive(theirs(3, zz), core_recv.at[3, zz, 0])

        def lower(s, _):
            j = zz * SIDES + s
            block = jnp.dot(hidden[...], down_full[j], preferred_element_type=f32)
            ffn_own[j] = block[:rows]
            for peer in (2, 0, 1):
                ffn_send[peer, j] = block[(peer + 1) * rows : (peer + 2) * rows].astype(bf16)
                rs_copy(peer, j).start()
            return 0

        lax.fori_loop(0, SIDES, lower, 0)

    for rank in range(depth):
        def finish(s, _):
            j = order[rank] * SIDES + s
            lanes = pl.ds(pl.multiple_of(j * slab, slab), slab)
            summed = ffn_own[j]
            for peer in range(3):
                rs_copy(peer, j).wait_recv()
                summed = summed + ffn_recv[peer, j].astype(f32)
            result[:, lanes] = (middle[:, lanes].astype(f32) + summed).astype(bf16)
            return 0

        lax.fori_loop(0, SIDES, finish, 0)

    for when, make in flights:
        if when is None:
            make().wait_send()
        else:
            pl.when(when)(lambda make=make: make().wait_send())

    @pl.when(crossed)
    def _():
        pltpu.make_async_remote_copy(
            src_ref=mine(2, z), dst_ref=mine(2, z), send_sem=swap_send.at[0], recv_sem=swap_recv.at[0],
            device_id=swap, device_id_type=MESH,
        ).wait_send()

    def drain(j, _):
        mix_copy(j).wait_send()
        for peer in range(3):
            rs_copy(peer, j).wait_send()
        return 0

    lax.fori_loop(0, slabs, drain, 0)


def resident(
    n_fs, n_tp, resid, mix_gain, in_weight, conv_taps, recur_gate_w, input_gate_w, decay_rate,
    out_weight, mlp_gain, up_gate_w, up_val_w, ffn_taps, down_weight,
):
    depth = n_fs // SIDES
    rows, width = resid.shape
    slab, chans = in_weight.shape
    units = up_gate_w.shape[1]
    slabs = width // slab
    tiles = units // LANES
    gates = jnp.concatenate([pair_blocks(recur_gate_w), pair_blocks(input_gate_w)], axis=2)
    pad = lambda table: jnp.pad(table, ((0, 8 - table.shape[0]), (0, 0)))
    params = jnp.concatenate(
        [pad(jnp.concatenate([conv_taps, decay_rate[None]], axis=0)), pad(ffn_taps)], axis=1
    )
    bf16, f32 = jnp.bfloat16, jnp.float32
    vmem = pl.BlockSpec(memory_space=pltpu.VMEM)
    hbm = pl.BlockSpec(memory_space=pl.ANY)
    dma = pltpu.SemaphoreType.DMA
    return pl.pallas_call(
        functools.partial(resident_kernel, depth),
        out_shape=jax.ShapeDtypeStruct((rows, width), bf16),
        in_specs=[vmem] * 5 + [hbm] * 5,
        out_specs=vmem,
        scratch_shapes=[
            pltpu.VMEM((CORES, width, chans), bf16),
            pltpu.VMEM((slabs, CORES * chans, slab), bf16),
            pltpu.VMEM((tiles, width, 2 * LANES), bf16),
            pltpu.VMEM((slabs, units, slab), bf16),
            pltpu.VMEM((CORES,) + params.shape, f32),
            pltpu.VMEM((CORES,) + gates.shape, bf16),
            pltpu.VMEM((2 * rows, width), bf16),
            pltpu.VMEM((2 * rows, CORES * chans), bf16),
            pltpu.VMEM((2 * rows, CORES * chans), bf16),
            pltpu.VMEM((slabs, rows, slab), f32),
            pltpu.VMEM((slabs, rows, slab), bf16),
            pltpu.VMEM((slabs, rows, slab), bf16),
            pltpu.VMEM((rows, width), bf16),
            pltpu.VMEM((4 * rows, width), bf16),
            pltpu.VMEM((4 * rows, units), bf16),
            pltpu.VMEM((slabs, rows, slab), f32),
            pltpu.VMEM((3, slabs, rows, slab), bf16),
            pltpu.VMEM((3, slabs, rows, slab), bf16),
            dma((6,)),
            dma((4, depth)), dma((4, depth)), dma((4, depth)),
            dma((2, depth)), dma((2, depth)),
            dma((4, depth, 2)), dma((4, depth, 2)),
            dma((2,)), dma((2,)),
            dma((2,)), dma((2,)),
            dma((2,)),
            dma((slabs,)), dma((slabs,)),
            dma((2, 3)), dma((2, 3)),
            dma((3, slabs)), dma((3, slabs)),
        ],
        compiler_params=pltpu.CompilerParams(
            has_side_effects=True, vmem_limit_bytes=VMEM_BYTES
        ),
    )(
        resid, mix_gain.reshape(1, -1), mlp_gain.reshape(1, -1), params, gates,
        in_weight, out_weight, up_gate_w, up_val_w, down_weight,
    )


def solution(mesh):
    in_specs = (
        P(("fs", "tp"), None),
        P(),
        P("fs", "tp"),
        P(None, "tp"),
        P("tp", None, None),
        P("tp", None, None),
        P("tp"),
        P("tp", "fs"),
        P(),
        P("fs", "tp"),
        P("fs", "tp"),
        P(None, "tp"),
        P("tp", "fs"),
    )
    out_specs = P(("fs", "tp"), None)
    n_fs, n_tp = mesh.shape["fs"], mesh.shape["tp"]
    body = functools.partial(resident if fits(n_fs, n_tp) else shards, n_fs, n_tp)
    return jax.shard_map(body, mesh=mesh, in_specs=in_specs, out_specs=out_specs, check_vma=False)
```

```python
import functools

import jax
import jax.numpy as jnp
from jax import lax
from jax.experimental import pallas as pl
from jax.experimental.pallas import tpu as pltpu
from jax.sharding import PartitionSpec as P

GATE_BLOCK = 64
SEQ_LEN = 128
LANES = 128
CORES = 2


def rms_scale(rows_in, gain_vec):
    wide = rows_in.astype(jnp.float32)
    return wide * lax.rsqrt(jnp.mean(wide * wide, axis=-1, keepdims=True) + 1e-06) * gain_vec


def causal_taps(values, tap_weights):
    width = tap_weights.shape[0]
    length = values.shape[1]
    padded = jnp.pad(values, ((0, 0), (width - 1, 0), (0, 0)))
    summed = jnp.zeros_like(values)
    for tap_index in range(width):
        summed = summed + padded[:, tap_index : tap_index + length] * tap_weights[tap_index]
    return summed


def negative_expm1(arg):
    series = jnp.ones_like(arg)
    for order in range(8, 1, -1):
        series = 1.0 + arg * (1.0 / order) * series
    return jnp.where(arg > -0.5, -arg * series, 1.0 - jnp.exp(arg))


def shift_rows(values, distance, rows, fill):
    return jnp.where(rows >= distance, pltpu.roll(values, distance, 0), fill)


def recurrence_kernel(projected_ref, taps_ref, gates_ref, rate_ref, out_ref):
    width = taps_ref.shape[0]
    rows = lax.broadcasted_iota(jnp.int32, (SEQ_LEN, LANES), 0)
    for chunk in range(projected_ref.shape[1] // LANES):
        cols = slice(chunk * LANES, (chunk + 1) * LANES)
        values = projected_ref[:, cols].astype(jnp.float32)
        conv = values * taps_ref[width - 1 : width, cols]
        for back in range(1, width):
            tap = taps_ref[width - 1 - back : width - back, cols]
            conv = conv + shift_rows(values, back, rows, 0.0) * tap
        gates = jax.nn.sigmoid(
            jnp.dot(
                conv.astype(jnp.bfloat16), gates_ref[chunk], preferred_element_type=jnp.float32
            )
        )
        rgate = gates[:, :LANES]
        igate = gates[:, LANES:]
        logdecay = -8.0 * rgate * rate_ref[:, cols]
        decay = jnp.exp(logdecay)
        state = jnp.sqrt(negative_expm1(2.0 * logdecay)) * (igate * conv)
        distance = 1
        while distance < SEQ_LEN:
            state = state + decay * shift_rows(state, distance, rows, 0.0)
            if 2 * distance < SEQ_LEN:
                decay = decay * shift_rows(decay, distance, rows, 1.0)
            distance *= 2
        out_ref[:, cols] = state.astype(jnp.bfloat16)


def pair_blocks(blocks):
    pairs = blocks.reshape(-1, 2, GATE_BLOCK, GATE_BLOCK)
    blank = jnp.zeros_like(pairs[:, 0])
    upper = jnp.concatenate([pairs[:, 0], blank], axis=2)
    lower = jnp.concatenate([blank, pairs[:, 1]], axis=2)
    return jnp.concatenate([upper, lower], axis=1)


def recurrence(projected, conv_taps, gates, decay_rate):
    count, channels = projected.shape
    whole = lambda shape: pl.BlockSpec(shape, lambda seq: (0,) * len(shape))
    return pl.pallas_call(
        recurrence_kernel,
        grid=(count // SEQ_LEN,),
        in_specs=[
            pl.BlockSpec((SEQ_LEN, channels), lambda seq: (seq, 0)),
            whole(conv_taps.shape),
            whole(gates.shape),
            whole((1, channels)),
        ],
        out_specs=pl.BlockSpec((SEQ_LEN, channels), lambda seq: (seq, 0)),
        out_shape=jax.ShapeDtypeStruct(projected.shape, jnp.bfloat16),
        cost_estimate=pl.CostEstimate(
            flops=count * channels * 600, bytes_accessed=count * channels * 4,
            transcendentals=count * channels * 6,
        ),
    )(projected, conv_taps, gates, decay_rate.reshape(1, channels))


def gather_groups(block, n_tp):
    sides = n_tp // CORES
    swap = [(i, i ^ 1) for i in range(n_tp)]
    groups = []
    for distance in range(sides):
        mine = block
        if distance:
            back = [
                (i, ((i // CORES - distance) % sides) * CORES + i % CORES) for i in range(n_tp)
            ]
            mine = lax.ppermute(block, "tp", back)
        groups.append(jnp.concatenate([mine, lax.ppermute(mine, "tp", swap)], axis=0))
    return groups


def scatter_sum(partial_of, n_tp):
    sides = n_tp // CORES
    swap = [(i, i ^ 1) for i in range(n_tp)]
    total = 0.0
    for distance in reversed(range(sides)):
        partial = partial_of(distance)
        half = partial.shape[0] // 2
        other = lax.ppermute(partial[half:], "tp", swap)
        pair = partial[:half].astype(jnp.float32) + other.astype(jnp.float32)
        if distance:
            ahead = [
                (i, ((i // CORES + distance) % sides) * CORES + i % CORES) for i in range(n_tp)
            ]
            pair = lax.ppermute(pair.astype(jnp.bfloat16), "tp", ahead).astype(jnp.float32)
        total = total + pair
    return total


def gather_weight(block, n_fs, n_tp):
    inner = n_tp // CORES if n_fs % (n_tp // CORES) == 0 else 1
    outer = n_fs // inner
    me = lax.axis_index("fs")
    parts = [block]
    for distance in range(1, outer):
        back = [(i, (i - distance * inner) % n_fs) for i in range(n_fs)]
        parts.append(lax.ppermute(block, "fs", back))
    start = lax.rem(outer - me // inner, outer)
    column = lax.dynamic_slice_in_dim(jnp.stack(parts + parts[:-1]), start, outer, 0)
    parts = [column]
    for distance in range(1, inner):
        back = [(i, i // inner * inner + (i - distance) % inner) for i in range(n_fs)]
        parts.append(lax.ppermute(column, "fs", back))
    start = lax.rem(inner - lax.rem(me, inner), inner)
    stacked = jnp.stack(parts + parts[:-1], axis=1)
    stacked = lax.dynamic_slice_in_dim(stacked, start, inner, 1)
    return stacked.reshape((n_fs,) + block.shape)


def side_by_side(stacked):
    return jnp.transpose(stacked, (1, 0, 2)).reshape(stacked.shape[1], -1)


def dot(left, right):
    return jnp.dot(left, right, preferred_element_type=jnp.float32).astype(jnp.bfloat16)


def shards(
    n_fs,
    n_tp,
    resid,
    mix_gain,
    in_weight,
    conv_taps,
    recur_gate_w,
    input_gate_w,
    decay_rate,
    out_weight,
    mlp_gain,
    up_gate_w,
    up_val_w,
    ffn_taps,
    down_weight,
):
    gate_full = lax.all_gather(up_gate_w, "fs", axis=0, tiled=True)
    val_full = lax.all_gather(up_val_w, "fs", axis=0, tiled=True)
    cut = down_weight.shape[0] - down_weight.shape[0] // (2 * LANES) * LANES
    down_head = lax.all_gather(down_weight[:cut], "fs", axis=1, tiled=True)
    in_full = gather_weight(in_weight, n_fs, n_tp).reshape(-1, in_weight.shape[1])
    out_full = side_by_side(gather_weight(out_weight, n_fs, n_tp))
    later = lax.optimization_barrier((down_weight[cut:], in_full))[0]
    down_tail = side_by_side(gather_weight(later, n_fs, n_tp))
    gates = jnp.concatenate([pair_blocks(recur_gate_w), pair_blocks(input_gate_w)], axis=2)

    normed = rms_scale(resid, mix_gain).astype(jnp.bfloat16)
    recurred = [
        recurrence(dot(rows, in_full), conv_taps, gates, decay_rate)
        for rows in gather_groups(normed, n_tp)
    ]
    mixed_sum = scatter_sum(lambda distance: dot(recurred[distance], out_full), n_tp)
    middle = (resid.astype(jnp.float32) + mixed_sum).astype(jnp.bfloat16)
    normed_two = rms_scale(middle, mlp_gain).astype(jnp.bfloat16)

    hidden = []
    for rows in gather_groups(normed_two, n_tp):
        gate_pre = dot(rows, gate_full)
        value_pre = dot(rows, val_full)
        seqs = gate_pre.shape[0] // SEQ_LEN
        gate_conv = causal_taps(
            gate_pre.astype(jnp.float32).reshape(seqs, SEQ_LEN, -1), ffn_taps
        ).reshape(gate_pre.shape)
        hidden.append((jax.nn.silu(gate_conv) * value_pre.astype(jnp.float32)).astype(jnp.bfloat16))
    tails = [
        jnp.dot(rows[:, cut:], down_tail, preferred_element_type=jnp.float32) for rows in hidden
    ]

    def down_partial(distance):
        head = jnp.dot(hidden[distance][:, :cut], down_head, preferred_element_type=jnp.float32)
        return (head + tails[distance]).astype(jnp.bfloat16)

    ffn_sum = scatter_sum(down_partial, n_tp)
    return (middle.astype(jnp.float32) + ffn_sum).astype(jnp.bfloat16)


MESH = pl.DeviceIdType.MESH
SIDES = 2
VMEM_BYTES = 66_000_000


def fits(n_fs, n_tp):
    return n_tp == SIDES * CORES and n_fs % SIDES == 0 and n_fs >= 2 * SIDES


def line_order(depth, z):
    ranks = []
    for here in range(depth):
        up_first = here < depth / 2
        others = [p for p in range(depth) if p != here]
        others.sort(key=lambda p: (abs(p - here), (p < here) == up_first))
        ranks.append([here] + others)
    order = []
    for rank in range(depth):
        place = jnp.int32(0)
        for here in range(depth):
            place = jnp.where(z == here, ranks[here][rank], place)
        order.append(place)
    return order


def resident_kernel(
    depth,
    resid_in, gain_one, gain_two, conv_taps, decay_rate, ffn_taps, recur_gate, input_gate,
    in_w, out_w, gate_w, val_w, down_w,
    result,
    resid, in_full, out_full, up_full, down_full, param_full, gate_full,
    normed, proj, recurred, mix_own, mix_send, mix_recv, middle, rows_two, hidden,
    ffn_own, ffn_next, pair_out, pair_in, last_out, last_in,
    local_sem, line_up, line_down, line_recv, side_send, side_recv, core_send, core_recv,
    swap_send, swap_recv, small_send, small_recv, row_sems, mix_sems_s, mix_sems_r,
    ag_send, ag_recv, pair_sems_s, pair_sems_r, last_sems_s, last_sems_r,
):
    f32, bf16 = jnp.float32, jnp.bfloat16
    fs, tp = lax.axis_index("fs"), lax.axis_index("tp")
    z, x = fs // SIDES, lax.rem(fs, SIDES)
    y, c = tp // CORES, lax.rem(tp, CORES)
    rows, width = resid.shape
    slab, chans = in_w.shape
    taps, ffn_width = conv_taps.shape[0], ffn_taps.shape[0]
    tiles = gate_w.shape[1] // LANES
    slabs = width // slab
    n_seq = rows // SEQ_LEN
    order = line_order(depth, z)
    straight, crossed = x == c, x != c
    has_up, has_down = z < depth - 1, z > 0
    inner = jnp.logical_and(has_up, has_down)
    outer = jnp.logical_not(inner)
    near, far = range(1, min(3, depth)), range(3, depth)

    at = lambda zz, xx, yy, cc: (zz * SIDES + xx, yy * CORES + cc)
    up, down = at(z + 1, x, y, c), at(z - 1, x, y, c)
    side, core, swap = at(z, 1 - x, y, c), at(z, x, y, 1 - c), at(z, c, y, x)
    across = at(z, x, 1 - y, c)

    barrier = pltpu.get_barrier_semaphore()
    greet = lambda dev: pl.semaphore_signal(barrier, inc=1, device_id=dev, device_id_type=MESH)
    for dev in (side, core, across):
        greet(dev)
    for when, dev in ((has_up, up), (has_down, down), (crossed, swap)):
        pl.when(when)(functools.partial(greet, dev))
    one = lambda when: when.astype(jnp.int32)
    pl.semaphore_wait(barrier, 3 + one(has_up) + one(has_down) + one(crossed))

    flights = []

    def when_all(*conds):
        conds = [cond for cond in conds if cond is not None]
        return functools.reduce(jnp.logical_and, conds) if conds else None

    def remote(src, dst, ss, rs, dev):
        return pltpu.make_async_remote_copy(
            src_ref=src, dst_ref=dst, send_sem=ss, recv_sem=rs, device_id=dev, device_id_type=MESH
        )

    def send(src, dst, ss, rs, dev, when=None):
        make = functools.partial(remote, src, dst, ss, rs, dev)
        if when is None:
            make().start()
        else:
            pl.when(when)(lambda: make().start())
        flights.append((when, make))

    def arrive(dst, rs, when=None):
        wait = lambda: remote(dst, dst, rs, rs, core).wait_recv()
        if when is None:
            wait()
        else:
            pl.when(when)(wait)

    def row_slab(zz, xx):
        return pl.ds(pl.multiple_of((zz * SIDES + xx) * slab, slab), slab)

    def place(a, zz, xx, cc):
        if a == 0:
            return in_full.at[cc, row_slab(zz, xx), :]
        if a == 1:
            return out_full.at[zz * SIDES + xx, pl.ds(pl.multiple_of(cc * chans, chans), chans), :]
        if a == 2:
            return up_full.at[:, row_slab(zz, xx), :]
        return down_full.at[zz * SIDES + xx]

    def mine(a, zz):
        return place(a, zz, x, c) if a < 2 else place(a, zz, c, c)

    def theirs(a, zz):
        return place(a, zz, x, 1 - c) if a < 2 else place(a, zz, 1 - c, c)

    def along(a, zz, src=None, when=None, own=False):
        dst = mine(a, zz)
        src = dst if src is None else src
        ups = has_up if own else jnp.logical_and(zz < z, has_up)
        downs = has_down if own else jnp.logical_and(zz > z, has_down)
        send(src, dst, line_up.at[a, zz], line_recv.at[a, zz], up, when_all(ups, when))
        send(src, dst, line_down.at[a, zz], line_recv.at[a, zz], down, when_all(downs, when))

    def to_side(a, zz, src=None):
        dst = mine(a, zz)
        send(dst if src is None else src, dst, side_send.at[a, zz], side_recv.at[a, zz], side)

    def to_core(a, zz, src=None, when=None):
        dst = mine(a, zz)
        slot = x if a < 2 else 0
        send(dst if src is None else src, dst, core_send.at[a, zz, 0], core_recv.at[a, zz, slot], core, when)

    def line_step(a, rank, when=None):
        if rank >= depth:
            return
        zz = order[rank]
        arrive(mine(a, zz), line_recv.at[a, zz], when)
        along(a, zz, when=when)
        if a < 2:
            to_side(a, zz)
        to_core(a, zz, when=when)

    def side_step(a, rank):
        if rank >= depth:
            return
        zz = order[rank]
        dst = place(a, zz, 1 - x, c)
        arrive(dst, side_recv.at[a, zz])
        send(dst, dst, core_send.at[a, zz, 1], core_recv.at[a, zz, 1 - x], core)

    in_copy = pltpu.make_async_copy(in_w, mine(0, z), local_sem.at[0])
    out_copy = pltpu.make_async_copy(out_w, mine(1, z), local_sem.at[1])
    up_copy = pltpu.make_async_copy(mine(2, z), mine(2, z), local_sem.at[2])
    down_copy = pltpu.make_async_copy(down_w, mine(3, z), local_sem.at[3])
    resid_copy = pltpu.make_async_copy(resid_in, resid, local_sem.at[4])

    def up_parts():
        for tile in range(tiles):
            for half, weight in enumerate((gate_w, val_w)):
                yield (
                    weight.at[:, pl.ds(tile * LANES, LANES)],
                    up_full.at[tile, row_slab(z, x), pl.ds(half * LANES, LANES)],
                )

    resid_copy.start()
    along(0, z, src=in_w, own=True)
    to_side(0, z, src=in_w)
    to_core(0, z, src=in_w)
    in_copy.start()
    out_copy.start()

    param_full[c, 0:taps, 0:chans] = conv_taps[...]
    param_full[c, taps : taps + 1, 0:chans] = decay_rate[...]
    param_full[c, 0:ffn_width, chans:] = ffn_taps[...]
    spot = lambda axis: lax.broadcasted_iota(jnp.int32, (GATE_BLOCK, LANES), axis)
    for half in range(LANES // GATE_BLOCK):
        spread = (spot(0) + half * GATE_BLOCK == spot(1)).astype(f32).astype(bf16)
        for kind, blocks in enumerate((recur_gate, input_gate)):
            for pair in range(chans // LANES):
                gate_full[
                    c, pair, half * GATE_BLOCK : (half + 1) * GATE_BLOCK, kind * LANES : (kind + 1) * LANES
                ] = jnp.dot(blocks[2 * pair + half], spread, preferred_element_type=f32).astype(bf16)
    resid_copy.wait()
    wide = resid[...].astype(f32)
    scale = lax.rsqrt(jnp.mean(wide * wide, axis=-1, keepdims=True) + 1e-06)
    normed[0:rows, :] = (wide * scale * gain_one[...]).astype(bf16)
    for i, full in enumerate((param_full, gate_full)):
        send(full.at[c], full.at[c], small_send.at[i], small_recv.at[i], core)
    send(normed.at[pl.ds(0, rows), :], normed.at[pl.ds(rows, rows), :], row_sems.at[0], row_sems.at[1], across)

    @pl.when(straight)
    def _():
        for src, dst in up_parts():
            pltpu.make_async_copy(src, dst, local_sem.at[2]).start()
        down_copy.start()

    for rank in near:
        line_step(0, rank)
    along(1, z, src=out_w, own=True)
    to_core(1, z, src=out_w)
    side_step(0, 0)
    side_step(0, 1)
    for rank in far:
        line_step(0, rank)

    @pl.when(crossed)
    def _():
        for src, dst in up_parts():
            remote(src, dst, swap_send.at[0], swap_recv.at[0], swap).start()

    to_side(1, z, src=out_w)
    side_step(0, 2)
    for rank in near:
        line_step(1, rank)
    for rank in far:
        side_step(0, rank)
    in_copy.wait()
    out_copy.wait()
    for i, full in enumerate((param_full, gate_full)):
        arrive(full.at[1 - c], small_recv.at[i])
    for rank in range(depth):
        zz = order[rank]
        for xx in range(SIDES):
            arrive(place(0, zz, xx, 1 - c), core_recv.at[0, zz, xx])
    arrive(normed.at[pl.ds(rows, rows), :], row_sems.at[1])

    wide_n = 2 * LANES
    per = chans // wide_n

    def project(i, _):
        cc, h = i // per, lax.rem(i, per)
        lanes = pl.ds(pl.multiple_of(h * wide_n, wide_n), wide_n)
        to = pl.ds(pl.multiple_of(i * wide_n, wide_n), wide_n)
        proj[:, to] = jnp.dot(normed[...], in_full[cc, :, lanes], preferred_element_type=f32).astype(bf16)
        return 0

    lax.fori_loop(0, CORES * per, project, 0)

    for rank in far:
        line_step(1, rank)

    @pl.when(straight)
    def _():
        up_copy.wait()
        down_copy.wait()

    along(2, z, when=straight, own=True)
    to_core(2, z, when=straight)
    send(down_w, place(3, z, x, c), swap_send.at[1], swap_recv.at[1], swap, crossed)

    position = lax.broadcasted_iota(jnp.int32, (SEQ_LEN, LANES), 0)
    chan_tiles = chans // LANES

    def recur(seq):
        where = pl.ds(seq * SEQ_LEN, SEQ_LEN)

        def tile_step(i, _):
            cc, u = i // chan_tiles, lax.rem(i, chan_tiles)
            cols = pl.ds(pl.multiple_of(u * LANES, LANES), LANES)
            to = pl.ds(pl.multiple_of(i * LANES, LANES), LANES)
            values = proj[where, to].astype(f32)
            table = param_full[cc, 0 : taps + 1, cols]
            conv = values * table[taps - 1 : taps]
            for back in range(1, taps):
                conv = conv + shift_rows(values, back, position, 0.0) * table[taps - 1 - back : taps - back]
            both = jax.nn.sigmoid(jnp.dot(conv.astype(bf16), gate_full[cc, u], preferred_element_type=f32))
            logdecay = -8.0 * both[:, :LANES] * table[taps : taps + 1]
            decay = jnp.exp(logdecay)
            state = jnp.sqrt(negative_expm1(2.0 * logdecay)) * (both[:, LANES:] * conv)
            distance = 1
            while distance < SEQ_LEN:
                state = state + decay * shift_rows(state, distance, position, 0.0)
                if 2 * distance < SEQ_LEN:
                    decay = decay * shift_rows(decay, distance, position, 1.0)
                distance *= 2
            recurred[where, to] = state.astype(bf16)
            return 0

        lax.fori_loop(0, CORES * chan_tiles, tile_step, 0)

    for seq in reversed(range(2 * n_seq)):
        recur(seq)
        if seq < 2:
            side_step(1, 1 - seq)

    arrive(mine(2, z), swap_recv.at[0], crossed)
    along(2, z, when=crossed, own=True)
    to_core(2, z, when=crossed)

    def mix_copy(j):
        return remote(mix_send.at[j], mix_recv.at[j], mix_sems_s.at[j], mix_sems_r.at[j], across)

    for rank in range(depth):
        zz = order[rank]
        if rank >= 2:
            side_step(1, rank)
        for xx in range(SIDES):
            arrive(place(1, zz, xx, 1 - c), core_recv.at[1, zz, xx])

        def mix(s, _):
            j = zz * SIDES + s
            both = jnp.dot(recurred[...], out_full[j], preferred_element_type=f32)
            mix_send[j] = both[rows:].astype(bf16)
            mix_copy(j).start()
            mix_own[j] = both[:rows]
            return 0

        lax.fori_loop(0, SIDES, mix, 0)
        if rank == 1:
            with jax.named_scope("up1_straight"):
                line_step(2, 1, when=straight)
                line_step(2, 2, when=when_all(straight, inner))

    total = jnp.zeros((rows, 1), f32)
    for j in range(slabs):
        mix_copy(j).wait_recv()
        lanes = slice(j * slab, (j + 1) * slab)
        value = (resid[:, lanes].astype(f32) + (mix_own[j] + mix_recv[j].astype(f32))).astype(bf16)
        middle[:, lanes] = value
        value = value.astype(f32)
        total = total + jnp.sum(value * value, axis=-1, keepdims=True)
    scale = lax.rsqrt(total * (1.0 / width) + 1e-06)
    rows_two[0:rows, :] = (middle[...].astype(f32) * scale * gain_two[...]).astype(bf16)

    part = rows // 2
    where = lambda slot, half: rows_two.at[pl.ds(slot * rows + half * part, part), :]
    send(where(0, 1), where(1, 1), ag_send.at[0, 0], ag_recv.at[0, 0], side)
    send(where(0, 0), where(2, 0), ag_send.at[1, 0], ag_recv.at[1, 0], across)
    send(where(0, 0), where(1, 0), ag_send.at[0, 1], ag_recv.at[0, 1], side)
    send(where(0, 1), where(2, 1), ag_send.at[1, 1], ag_recv.at[1, 1], across)
    line_step(2, 1, when=crossed)
    line_step(2, 2, when=when_all(crossed, inner))
    arrive(where(1, 1), ag_recv.at[0, 0])
    send(where(1, 1), where(3, 1), ag_send.at[1, 2], ag_recv.at[1, 2], across)
    arrive(where(2, 0), ag_recv.at[1, 0])
    send(where(2, 0), where(3, 0), ag_send.at[0, 2], ag_recv.at[0, 2], side)
    for rank in far:
        line_step(2, rank, when=inner)
    arrive(mine(3, z), swap_recv.at[1], crossed)
    along(3, z, own=True)
    to_core(3, z)
    arrive(where(1, 0), ag_recv.at[0, 1])
    arrive(where(2, 1), ag_recv.at[1, 1])
    arrive(where(3, 0), ag_recv.at[0, 2])
    arrive(where(3, 1), ag_recv.at[1, 2])
    line_step(2, 2, when=outer)
    for rank in far:
        line_step(2, rank, when=outer)
    for rank in range(depth):
        arrive(theirs(2, order[rank]), core_recv.at[2, order[rank], 0])

    lift = 2 * rows
    row_in_seq = lax.rem(lax.broadcasted_iota(jnp.int32, (lift, LANES), 0), SEQ_LEN)

    def raise_tile(t, _):
        cols = pl.ds(pl.multiple_of(t * LANES, LANES), LANES)
        table = param_full[x, 0:ffn_width, pl.ds(pl.multiple_of(chans + t * LANES, LANES), LANES)]
        for block in range(2):
            here = slice(block * lift, (block + 1) * lift)
            pre = jnp.dot(rows_two[here, :], up_full[t], preferred_element_type=f32)
            gate = pre[:, :LANES].astype(bf16).astype(f32)
            value = pre[:, LANES:].astype(bf16).astype(f32)
            conv = gate * table[ffn_width - 1 : ffn_width]
            for back in range(1, ffn_width):
                shifted = shift_rows(gate, back, row_in_seq, 0.0)
                conv = conv + shifted * table[ffn_width - 1 - back : ffn_width - back]
            hidden[here, cols] = (jax.nn.silu(conv) * value).astype(bf16)
        return 0

    first = tiles // 2
    lax.fori_loop(0, first, raise_tile, 0)
    for rank in near:
        line_step(3, rank, when=inner)
    lax.fori_loop(first, tiles, raise_tile, 0)

    def first_leg(j, s):
        return remote(pair_out.at[j], pair_in.at[j], pair_sems_s.at[j], pair_sems_r.at[j], (side, across)[s])

    def last_leg(j, s):
        return remote(last_out.at[j], last_in.at[j], last_sems_s.at[j], last_sems_r.at[j], (across, side)[s])

    def pass_on(rank):
        for s in range(SIDES):
            j = order[rank] * SIDES + s
            first_leg(j, s).wait_recv()
            last_out[j] = (ffn_next[j] + pair_in[j, 1].astype(f32)).astype(bf16)
            ffn_own[j] = ffn_own[j] + pair_in[j, 0].astype(f32)
            last_leg(j, s).start()

    for rank in range(depth):
        zz = order[rank]
        with jax.named_scope("dstep"):
            if rank in near:
                line_step(3, rank, when=outer)
            elif rank:
                line_step(3, rank)
        with jax.named_scope("dcore"):
            arrive(theirs(3, zz), core_recv.at[3, zz, 0])
        for s in range(SIDES):
            j = zz * SIDES + s
            block = jnp.dot(hidden[...], down_full[j], preferred_element_type=f32)
            beside, beyond = ((1, 2), (2, 1))[s]
            part_of = lambda slot: block[slot * rows : (slot + 1) * rows]
            pair_out[j, 0] = part_of(beside).astype(bf16)
            pair_out[j, 1] = part_of(3).astype(bf16)
            first_leg(j, s).start()
            ffn_own[j] = part_of(0)
            ffn_next[j] = part_of(beyond)
        if rank:
            pass_on(rank - 1)
    pass_on(depth - 1)

    for rank in range(depth):
        for s in range(SIDES):
            j = order[rank] * SIDES + s
            lanes = pl.ds(pl.multiple_of(j * slab, slab), slab)
            last_leg(j, s).wait_recv()
            summed = ffn_own[j] + last_in[j].astype(f32)
            result[:, lanes] = (middle[:, lanes].astype(f32) + summed).astype(bf16)

    for when, make in flights:
        if when is None:
            make().wait_send()
        else:
            pl.when(when)(lambda make=make: make().wait_send())

    @pl.when(crossed)
    def _():
        remote(mine(2, z), mine(2, z), swap_send.at[0], swap_recv.at[0], swap).wait_send()

    for rank in range(depth):
        for s in range(SIDES):
            j = order[rank] * SIDES + s
            mix_copy(j).wait_send()
            first_leg(j, s).wait_send()
            last_leg(j, s).wait_send()


def resident(
    n_fs, n_tp, resid, mix_gain, in_weight, conv_taps, recur_gate_w, input_gate_w, decay_rate,
    out_weight, mlp_gain, up_gate_w, up_val_w, ffn_taps, down_weight,
):
    depth = n_fs // SIDES
    rows, width = resid.shape
    slab, chans = in_weight.shape
    units = up_gate_w.shape[1]
    slabs = width // slab
    tiles = units // LANES
    bf16, f32 = jnp.bfloat16, jnp.float32
    vmem = pl.BlockSpec(memory_space=pltpu.VMEM)
    hbm = pl.BlockSpec(memory_space=pl.ANY)
    dma = pltpu.SemaphoreType.DMA
    return pl.pallas_call(
        functools.partial(resident_kernel, depth),
        out_shape=jax.ShapeDtypeStruct((rows, width), bf16),
        in_specs=[hbm] + [vmem] * 7 + [hbm] * 5,
        out_specs=vmem,
        scratch_shapes=[
            pltpu.VMEM((rows, width), bf16),
            pltpu.VMEM((CORES, width, chans), bf16),
            pltpu.VMEM((slabs, CORES * chans, slab), bf16),
            pltpu.VMEM((tiles, width, 2 * LANES), bf16),
            pltpu.VMEM((slabs, units, slab), bf16),
            pltpu.VMEM((CORES, 8, chans + units), f32),
            pltpu.VMEM((CORES, chans // LANES, LANES, 2 * LANES), bf16),
            pltpu.VMEM((2 * rows, width), bf16),
            pltpu.VMEM((2 * rows, CORES * chans), bf16),
            pltpu.VMEM((2 * rows, CORES * chans), bf16),
            pltpu.VMEM((slabs, rows, slab), f32),
            pltpu.VMEM((slabs, rows, slab), bf16),
            pltpu.VMEM((slabs, rows, slab), bf16),
            pltpu.VMEM((rows, width), bf16),
            pltpu.VMEM((4 * rows, width), bf16),
            pltpu.VMEM((4 * rows, units), bf16),
            pltpu.VMEM((slabs, rows, slab), f32),
            pltpu.VMEM((slabs, rows, slab), f32),
            pltpu.VMEM((slabs, 2, rows, slab), bf16),
            pltpu.VMEM((slabs, 2, rows, slab), bf16),
            pltpu.VMEM((slabs, rows, slab), bf16),
            pltpu.VMEM((slabs, rows, slab), bf16),
            dma((5,)),
            dma((4, depth)), dma((4, depth)), dma((4, depth)),
            dma((2, depth)), dma((2, depth)),
            dma((4, depth, 2)), dma((4, depth, 2)),
            dma((2,)), dma((2,)),
            dma((2,)), dma((2,)),
            dma((2,)),
            dma((slabs,)), dma((slabs,)),
            dma((2, 3)), dma((2, 3)),
            dma((slabs,)), dma((slabs,)), dma((slabs,)), dma((slabs,)),
        ],
        compiler_params=pltpu.CompilerParams(
            collective_id=0, has_side_effects=True, vmem_limit_bytes=VMEM_BYTES
        ),
    )(
        resid, mix_gain.reshape(1, -1), mlp_gain.reshape(1, -1), conv_taps, decay_rate.reshape(1, -1),
        ffn_taps, recur_gate_w, input_gate_w, in_weight, out_weight, up_gate_w, up_val_w, down_weight,
    )


def solution(mesh):
    in_specs = (
        P(("fs", "tp"), None),
        P(),
        P("fs", "tp"),
        P(None, "tp"),
        P("tp", None, None),
        P("tp", None, None),
        P("tp"),
        P("tp", "fs"),
        P(),
        P("fs", "tp"),
        P("fs", "tp"),
        P(None, "tp"),
        P("tp", "fs"),
    )
    out_specs = P(("fs", "tp"), None)
    n_fs, n_tp = mesh.shape["fs"], mesh.shape["tp"]
    body = functools.partial(resident if fits(n_fs, n_tp) else shards, n_fs, n_tp)
    return jax.shard_map(body, mesh=mesh, in_specs=in_specs, out_specs=out_specs, check_vma=False)
```

```python
import functools

import jax
import jax.numpy as jnp
from jax import lax
from jax.experimental import pallas as pl
from jax.experimental.pallas import tpu as pltpu
from jax.sharding import PartitionSpec as P

GATE_BLOCK = 64
SEQ_LEN = 128
LANES = 128
CORES = 2


def rms_scale(rows_in, gain_vec):
    wide = rows_in.astype(jnp.float32)
    return wide * lax.rsqrt(jnp.mean(wide * wide, axis=-1, keepdims=True) + 1e-06) * gain_vec


def causal_taps(values, tap_weights):
    width = tap_weights.shape[0]
    length = values.shape[1]
    padded = jnp.pad(values, ((0, 0), (width - 1, 0), (0, 0)))
    summed = jnp.zeros_like(values)
    for tap_index in range(width):
        summed = summed + padded[:, tap_index : tap_index + length] * tap_weights[tap_index]
    return summed


def negative_expm1(arg):
    series = jnp.ones_like(arg)
    for order in range(8, 1, -1):
        series = 1.0 + arg * (1.0 / order) * series
    return jnp.where(arg > -0.5, -arg * series, 1.0 - jnp.exp(arg))


def shift_rows(values, distance, rows, fill):
    return jnp.where(rows >= distance, pltpu.roll(values, distance, 0), fill)


def recurrence_kernel(projected_ref, taps_ref, gates_ref, rate_ref, out_ref):
    width = taps_ref.shape[0]
    rows = lax.broadcasted_iota(jnp.int32, (SEQ_LEN, LANES), 0)
    for chunk in range(projected_ref.shape[1] // LANES):
        cols = slice(chunk * LANES, (chunk + 1) * LANES)
        values = projected_ref[:, cols].astype(jnp.float32)
        conv = values * taps_ref[width - 1 : width, cols]
        for back in range(1, width):
            tap = taps_ref[width - 1 - back : width - back, cols]
            conv = conv + shift_rows(values, back, rows, 0.0) * tap
        gates = jax.nn.sigmoid(
            jnp.dot(
                conv.astype(jnp.bfloat16), gates_ref[chunk], preferred_element_type=jnp.float32
            )
        )
        rgate = gates[:, :LANES]
        igate = gates[:, LANES:]
        logdecay = -8.0 * rgate * rate_ref[:, cols]
        decay = jnp.exp(logdecay)
        state = jnp.sqrt(negative_expm1(2.0 * logdecay)) * (igate * conv)
        distance = 1
        while distance < SEQ_LEN:
            state = state + decay * shift_rows(state, distance, rows, 0.0)
            if 2 * distance < SEQ_LEN:
                decay = decay * shift_rows(decay, distance, rows, 1.0)
            distance *= 2
        out_ref[:, cols] = state.astype(jnp.bfloat16)


def pair_blocks(blocks):
    pairs = blocks.reshape(-1, 2, GATE_BLOCK, GATE_BLOCK)
    blank = jnp.zeros_like(pairs[:, 0])
    upper = jnp.concatenate([pairs[:, 0], blank], axis=2)
    lower = jnp.concatenate([blank, pairs[:, 1]], axis=2)
    return jnp.concatenate([upper, lower], axis=1)


def recurrence(projected, conv_taps, gates, decay_rate):
    count, channels = projected.shape
    whole = lambda shape: pl.BlockSpec(shape, lambda seq: (0,) * len(shape))
    return pl.pallas_call(
        recurrence_kernel,
        grid=(count // SEQ_LEN,),
        in_specs=[
            pl.BlockSpec((SEQ_LEN, channels), lambda seq: (seq, 0)),
            whole(conv_taps.shape),
            whole(gates.shape),
            whole((1, channels)),
        ],
        out_specs=pl.BlockSpec((SEQ_LEN, channels), lambda seq: (seq, 0)),
        out_shape=jax.ShapeDtypeStruct(projected.shape, jnp.bfloat16),
        cost_estimate=pl.CostEstimate(
            flops=count * channels * 600, bytes_accessed=count * channels * 4,
            transcendentals=count * channels * 6,
        ),
    )(projected, conv_taps, gates, decay_rate.reshape(1, channels))


def gather_groups(block, n_tp):
    sides = n_tp // CORES
    swap = [(i, i ^ 1) for i in range(n_tp)]
    groups = []
    for distance in range(sides):
        mine = block
        if distance:
            back = [
                (i, ((i // CORES - distance) % sides) * CORES + i % CORES) for i in range(n_tp)
            ]
            mine = lax.ppermute(block, "tp", back)
        groups.append(jnp.concatenate([mine, lax.ppermute(mine, "tp", swap)], axis=0))
    return groups


def scatter_sum(partial_of, n_tp):
    sides = n_tp // CORES
    swap = [(i, i ^ 1) for i in range(n_tp)]
    total = 0.0
    for distance in reversed(range(sides)):
        partial = partial_of(distance)
        half = partial.shape[0] // 2
        other = lax.ppermute(partial[half:], "tp", swap)
        pair = partial[:half].astype(jnp.float32) + other.astype(jnp.float32)
        if distance:
            ahead = [
                (i, ((i // CORES + distance) % sides) * CORES + i % CORES) for i in range(n_tp)
            ]
            pair = lax.ppermute(pair.astype(jnp.bfloat16), "tp", ahead).astype(jnp.float32)
        total = total + pair
    return total


def gather_weight(block, n_fs, n_tp):
    inner = n_tp // CORES if n_fs % (n_tp // CORES) == 0 else 1
    outer = n_fs // inner
    me = lax.axis_index("fs")
    parts = [block]
    for distance in range(1, outer):
        back = [(i, (i - distance * inner) % n_fs) for i in range(n_fs)]
        parts.append(lax.ppermute(block, "fs", back))
    start = lax.rem(outer - me // inner, outer)
    column = lax.dynamic_slice_in_dim(jnp.stack(parts + parts[:-1]), start, outer, 0)
    parts = [column]
    for distance in range(1, inner):
        back = [(i, i // inner * inner + (i - distance) % inner) for i in range(n_fs)]
        parts.append(lax.ppermute(column, "fs", back))
    start = lax.rem(inner - lax.rem(me, inner), inner)
    stacked = jnp.stack(parts + parts[:-1], axis=1)
    stacked = lax.dynamic_slice_in_dim(stacked, start, inner, 1)
    return stacked.reshape((n_fs,) + block.shape)


def side_by_side(stacked):
    return jnp.transpose(stacked, (1, 0, 2)).reshape(stacked.shape[1], -1)


def dot(left, right):
    return jnp.dot(left, right, preferred_element_type=jnp.float32).astype(jnp.bfloat16)


def shards(
    n_fs,
    n_tp,
    resid,
    mix_gain,
    in_weight,
    conv_taps,
    recur_gate_w,
    input_gate_w,
    decay_rate,
    out_weight,
    mlp_gain,
    up_gate_w,
    up_val_w,
    ffn_taps,
    down_weight,
):
    gate_full = lax.all_gather(up_gate_w, "fs", axis=0, tiled=True)
    val_full = lax.all_gather(up_val_w, "fs", axis=0, tiled=True)
    cut = down_weight.shape[0] - down_weight.shape[0] // (2 * LANES) * LANES
    down_head = lax.all_gather(down_weight[:cut], "fs", axis=1, tiled=True)
    in_full = gather_weight(in_weight, n_fs, n_tp).reshape(-1, in_weight.shape[1])
    out_full = side_by_side(gather_weight(out_weight, n_fs, n_tp))
    later = lax.optimization_barrier((down_weight[cut:], in_full))[0]
    down_tail = side_by_side(gather_weight(later, n_fs, n_tp))
    gates = jnp.concatenate([pair_blocks(recur_gate_w), pair_blocks(input_gate_w)], axis=2)

    normed = rms_scale(resid, mix_gain).astype(jnp.bfloat16)
    recurred = [
        recurrence(dot(rows, in_full), conv_taps, gates, decay_rate)
        for rows in gather_groups(normed, n_tp)
    ]
    mixed_sum = scatter_sum(lambda distance: dot(recurred[distance], out_full), n_tp)
    middle = (resid.astype(jnp.float32) + mixed_sum).astype(jnp.bfloat16)
    normed_two = rms_scale(middle, mlp_gain).astype(jnp.bfloat16)

    hidden = []
    for rows in gather_groups(normed_two, n_tp):
        gate_pre = dot(rows, gate_full)
        value_pre = dot(rows, val_full)
        seqs = gate_pre.shape[0] // SEQ_LEN
        gate_conv = causal_taps(
            gate_pre.astype(jnp.float32).reshape(seqs, SEQ_LEN, -1), ffn_taps
        ).reshape(gate_pre.shape)
        hidden.append((jax.nn.silu(gate_conv) * value_pre.astype(jnp.float32)).astype(jnp.bfloat16))
    tails = [
        jnp.dot(rows[:, cut:], down_tail, preferred_element_type=jnp.float32) for rows in hidden
    ]

    def down_partial(distance):
        head = jnp.dot(hidden[distance][:, :cut], down_head, preferred_element_type=jnp.float32)
        return (head + tails[distance]).astype(jnp.bfloat16)

    ffn_sum = scatter_sum(down_partial, n_tp)
    return (middle.astype(jnp.float32) + ffn_sum).astype(jnp.bfloat16)


MESH = pl.DeviceIdType.MESH
SIDES = 2
VMEM_BYTES = 66_000_000


def fits(n_fs, n_tp):
    return n_tp == SIDES * CORES and n_fs % SIDES == 0 and n_fs >= 2 * SIDES


def line_order(depth, z):
    ranks = []
    for here in range(depth):
        up_first = here < depth / 2
        others = [p for p in range(depth) if p != here]
        others.sort(key=lambda p: (abs(p - here), (p < here) == up_first))
        ranks.append([here] + others)
    order = []
    for rank in range(depth):
        place = jnp.int32(0)
        for here in range(depth):
            place = jnp.where(z == here, ranks[here][rank], place)
        order.append(place)
    return order


def resident_kernel(
    depth,
    resid_in, gain_one, gain_two, conv_taps, decay_rate, ffn_taps, recur_gate, input_gate,
    in_w, out_w, gate_w, val_w, down_w,
    result,
    resid, in_full, out_full, up_full, down_full, param_full, gate_full,
    normed, proj, recurred, mix_own, mix_send, mix_recv, middle, rows_two, hidden,
    sums, ffn_next, pair_out, pair_in, last_out, last_in, made,
    local_sem, line_send, line_twin, line_recv, side_send, side_recv, core_send, core_recv,
    swap_send, swap_recv, small_send, small_recv, row_sems, mix_recv_sem, ag_recv,
    pair_sem, pair_half, last_sem, last_half, bulk,
):
    f32, bf16 = jnp.float32, jnp.bfloat16
    fs, tp = lax.axis_index("fs"), lax.axis_index("tp")
    z, x = fs // SIDES, lax.rem(fs, SIDES)
    y, c = tp // CORES, lax.rem(tp, CORES)
    rows, width = resid.shape
    slab, chans = in_w.shape
    taps, ffn_width = conv_taps.shape[0], ffn_taps.shape[0]
    tiles = gate_w.shape[1] // LANES
    slabs = width // slab
    n_seq = rows // SEQ_LEN
    order = line_order(depth, z)
    straight, crossed = x == c, x != c
    has_up, has_down = z < depth - 1, z > 0
    inner = jnp.logical_and(has_up, has_down)
    outer = jnp.logical_not(inner)
    near, far = range(1, min(3, depth)), range(3, depth)

    at = lambda zz, xx, yy, cc: (zz * SIDES + xx, yy * CORES + cc)
    up, down = at(z + 1, x, y, c), at(z - 1, x, y, c)
    side, core, swap = at(z, 1 - x, y, c), at(z, x, y, 1 - c), at(z, c, y, x)
    across = at(z, x, 1 - y, c)

    barrier = pltpu.get_barrier_semaphore()
    greet = lambda dev: pl.semaphore_signal(barrier, inc=1, device_id=dev, device_id_type=MESH)
    for dev in (side, core, across):
        greet(dev)
    for when, dev in ((has_up, up), (has_down, down), (crossed, swap)):
        pl.when(when)(functools.partial(greet, dev))
    one = lambda when: when.astype(jnp.int32)
    pl.semaphore_wait(barrier, 3 + one(has_up) + one(has_down) + one(crossed))

    flights = []

    def when_all(*conds):
        conds = [cond for cond in conds if cond is not None]
        return functools.reduce(jnp.logical_and, conds) if conds else None

    def remote(src, dst, ss, rs, dev):
        return pltpu.make_async_remote_copy(
            src_ref=src, dst_ref=dst, send_sem=ss, recv_sem=rs, device_id=dev, device_id_type=MESH
        )

    def send(src, dst, ss, rs, dev, when=None, alone=True):
        make = functools.partial(remote, src, dst, ss, rs, dev)
        if when is None:
            make().start()
        else:
            pl.when(when)(lambda: make().start())
        if alone:
            flights.append((when, make))

    def gone(whole, ss):
        remote(whole, whole, ss, ss, core).wait_send()

    def arrive(dst, rs, when=None):
        wait = lambda: remote(dst, dst, rs, rs, core).wait_recv()
        if when is None:
            wait()
        else:
            pl.when(when)(wait)

    def row_slab(zz, xx):
        return pl.ds(pl.multiple_of((zz * SIDES + xx) * slab, slab), slab)

    def place(a, zz, xx, cc):
        if a == 0:
            return in_full.at[cc, row_slab(zz, xx), :]
        if a == 1:
            return out_full.at[zz * SIDES + xx, pl.ds(pl.multiple_of(cc * chans, chans), chans), :]
        if a == 2:
            return up_full.at[zz * SIDES + xx]
        return down_full.at[zz * SIDES + xx, a - 3]

    def mine(a, zz):
        return place(a, zz, x, c) if a < 2 else place(a, zz, c, c)

    def theirs(a, zz):
        return place(a, zz, x, 1 - c) if a < 2 else place(a, zz, 1 - c, c)

    def along(a, zz, src=None, when=None, own=False):
        dst = mine(a, zz)
        src = dst if src is None else src
        ups = has_up if own else jnp.logical_and(zz < z, has_up)
        downs = has_down if own else jnp.logical_and(zz > z, has_down)
        twin = line_twin.at[a] if own else line_send.at[a, zz]
        send(src, dst, line_send.at[a, zz], line_recv.at[a, zz], up, when_all(ups, when))
        send(src, dst, twin, line_recv.at[a, zz], down, when_all(downs, when))

    def to_side(a, zz, src=None, when=None):
        dst = mine(a, zz)
        send(dst if src is None else src, dst, side_send.at[a], side_recv.at[a, zz], side, when, False)

    def core_sem(a, zz):
        return core_recv.at[a, 0] if a == 0 else core_recv.at[a, zz]

    def to_core(a, zz, src=None, when=None):
        dst = mine(a, zz)
        send(dst if src is None else src, dst, core_send.at[a], core_sem(a, zz), core, when, False)

    def line_step(a, rank, when=None):
        if rank >= depth:
            return
        zz = order[rank]
        arrive(mine(a, zz), line_recv.at[a, zz], when)
        along(a, zz, when=when)
        if a < 2:
            to_side(a, zz, when=when_all(when, (None, crossed)[a]))
        to_core(a, zz, when=when)

    def side_step(a, rank):
        if rank >= depth:
            return
        zz = order[rank]
        dst = place(a, zz, 1 - x, c)
        arrive(dst, side_recv.at[a, zz])
        send(dst, dst, core_send.at[a], core_sem(a, zz), core, None, False)

    in_copy = pltpu.make_async_copy(in_w, mine(0, z), local_sem.at[0])
    out_copy = pltpu.make_async_copy(out_w, mine(1, z), local_sem.at[1])
    up_copy = pltpu.make_async_copy(mine(2, z), mine(2, z), local_sem.at[2])
    thin = slab // 2
    down_part = lambda h: down_w.at[:, pl.ds(h * thin, thin)]
    down_copies = [pltpu.make_async_copy(down_part(h), mine(3 + h, z), local_sem.at[3 + h]) for h in range(2)]
    resid_copy = pltpu.make_async_copy(resid_in, resid, local_sem.at[5])

    def up_parts():
        for tile in range(tiles):
            for half, weight in enumerate((gate_w, val_w)):
                yield (
                    weight.at[:, pl.ds(tile * LANES, LANES)],
                    up_full.at[z * SIDES + x, tile, :, pl.ds(half * LANES, LANES)],
                )

    resid_copy.start()
    along(0, z, src=in_w, own=True)
    to_side(0, z, src=in_w)
    to_core(0, z, src=in_w)
    in_copy.start()
    out_copy.start()

    param_full[c, 0:taps, 0:chans] = conv_taps[...]
    param_full[c, taps : taps + 1, 0:chans] = decay_rate[...]
    param_full[c, 0:ffn_width, chans:] = ffn_taps[...]
    spot = lambda axis: lax.broadcasted_iota(jnp.int32, (GATE_BLOCK, LANES), axis)
    for half in range(LANES // GATE_BLOCK):
        spread = (spot(0) + half * GATE_BLOCK == spot(1)).astype(f32).astype(bf16)
        for kind, blocks in enumerate((recur_gate, input_gate)):
            for pair in range(chans // LANES):
                gate_full[
                    c, pair, half * GATE_BLOCK : (half + 1) * GATE_BLOCK, kind * LANES : (kind + 1) * LANES
                ] = jnp.dot(blocks[2 * pair + half], spread, preferred_element_type=f32).astype(bf16)
    resid_copy.wait()
    wide = resid[...].astype(f32)
    scale = lax.rsqrt(jnp.mean(wide * wide, axis=-1, keepdims=True) + 1e-06)
    normed[0:rows, :] = (wide * scale * gain_one[...]).astype(bf16)
    for i, full in enumerate((param_full, gate_full)):
        send(full.at[c], full.at[c], small_send.at[i], small_recv.at[i], core)
    send(normed.at[pl.ds(0, rows), :], normed.at[pl.ds(rows, rows), :], row_sems.at[0], row_sems.at[1], across)

    @pl.when(straight)
    def _():
        for src, dst in up_parts():
            pltpu.make_async_copy(src, dst, local_sem.at[2]).start()
        for copy in down_copies:
            copy.start()

    for rank in near:
        line_step(0, rank)
    along(1, z, src=out_w, own=True)
    to_core(1, z, src=out_w)
    side_step(0, 0)
    side_step(0, 1)

    def swap_some(parts):
        @pl.when(crossed)
        def _():
            for src, dst in parts:
                remote(src, dst, swap_send.at[0], swap_recv.at[0], swap).start()

    parts = list(up_parts())
    swap_some(parts[:tiles])
    for rank in far:
        line_step(0, rank)
    swap_some(parts[tiles:])
    to_side(1, z, src=out_w, when=crossed)
    side_step(0, 2)
    for rank in near:
        line_step(1, rank)

    def out_and_up(when):
        for rank in far:
            line_step(1, rank, when=when)
        ready = jnp.logical_and(straight, when)

        @pl.when(ready)
        def _():
            up_copy.wait()
            for copy in down_copies:
                copy.wait()

        along(2, z, when=ready, own=True)
        to_core(2, z, when=ready)

    out_and_up(inner)
    for rank in far:
        side_step(0, rank)
    in_copy.wait()
    out_copy.wait()
    for i, full in enumerate((param_full, gate_full)):
        arrive(full.at[1 - c], small_recv.at[i])
    arrive(in_full.at[1 - c], core_recv.at[0, 0])
    arrive(normed.at[pl.ds(rows, rows), :], row_sems.at[1])

    wide_n = 2 * LANES
    per = chans // wide_n

    def project(i, _):
        cc, h = i // per, lax.rem(i, per)
        lanes = pl.ds(pl.multiple_of(h * wide_n, wide_n), wide_n)
        to = pl.ds(pl.multiple_of(i * wide_n, wide_n), wide_n)
        proj[:, to] = jnp.dot(normed[...], in_full[cc, :, lanes], preferred_element_type=f32).astype(bf16)
        return 0

    lax.fori_loop(0, CORES * per, project, 0)

    to_side(1, z, src=out_w, when=straight)
    for rank in near:
        to_side(1, order[rank], when=straight)
    out_and_up(outer)
    for rank in far:
        to_side(1, order[rank], when=straight)
    for h in range(2):
        send(down_part(h), place(3 + h, z, x, c), swap_send.at[1], swap_recv.at[1], swap, crossed, False)

    position = lax.broadcasted_iota(jnp.int32, (SEQ_LEN, LANES), 0)
    chan_tiles = chans // LANES

    def recur(seq):
        where = pl.ds(seq * SEQ_LEN, SEQ_LEN)

        def tile_step(i, _):
            cc, u = i // chan_tiles, lax.rem(i, chan_tiles)
            cols = pl.ds(pl.multiple_of(u * LANES, LANES), LANES)
            to = pl.ds(pl.multiple_of(i * LANES, LANES), LANES)
            values = proj[where, to].astype(f32)
            table = param_full[cc, 0 : taps + 1, cols]
            conv = values * table[taps - 1 : taps]
            for back in range(1, taps):
                conv = conv + shift_rows(values, back, position, 0.0) * table[taps - 1 - back : taps - back]
            both = jax.nn.sigmoid(jnp.dot(conv.astype(bf16), gate_full[cc, u], preferred_element_type=f32))
            logdecay = -8.0 * both[:, :LANES] * table[taps : taps + 1]
            decay = jnp.exp(logdecay)
            state = jnp.sqrt(negative_expm1(2.0 * logdecay)) * (both[:, LANES:] * conv)
            distance = 1
            while distance < SEQ_LEN:
                state = state + decay * shift_rows(state, distance, position, 0.0)
                if 2 * distance < SEQ_LEN:
                    decay = decay * shift_rows(decay, distance, position, 1.0)
                distance *= 2
            recurred[where, to] = state.astype(bf16)
            return 0

        lax.fori_loop(0, CORES * chan_tiles, tile_step, 0)

    for seq in reversed(range(2 * n_seq)):
        recur(seq)
        if seq < 2:
            side_step(1, 1 - seq)

    arrive(mine(2, z), swap_recv.at[0], crossed)
    along(2, z, when=crossed, own=True)
    to_core(2, z, when=crossed)

    def mix_copy(j):
        return remote(mix_send.at[j], mix_recv.at[j], bulk.at[0], mix_recv_sem.at[j], across)

    for rank in range(depth):
        zz = order[rank]
        if rank >= 2:
            side_step(1, rank)
        theirs_out = pl.ds(pl.multiple_of((1 - c) * chans, chans), chans)
        arrive(out_full.at[pl.ds(zz * SIDES, SIDES), theirs_out, :], core_recv.at[1, zz])

        def mix(s, _):
            j = zz * SIDES + s
            both = jnp.dot(recurred[...], out_full[j], preferred_element_type=f32)
            mix_send[j] = both[rows:].astype(bf16)
            mix_copy(j).start()
            mix_own[j] = both[:rows]
            return 0

        lax.fori_loop(0, SIDES, mix, 0)
        if rank == 1:
            with jax.named_scope("up1_straight"):
                line_step(2, 1, when=straight)
                line_step(2, 2, when=when_all(straight, inner))

    total = jnp.zeros((rows, 1), f32)
    for j in range(slabs):
        mix_copy(j).wait_recv()
        lanes = slice(j * slab, (j + 1) * slab)
        value = (resid[:, lanes].astype(f32) + (mix_own[j] + mix_recv[j].astype(f32))).astype(bf16)
        middle[:, lanes] = value
        value = value.astype(f32)
        total = total + jnp.sum(value * value, axis=-1, keepdims=True)
    scale = lax.rsqrt(total * (1.0 / width) + 1e-06)
    rows_two[0:rows, :] = (middle[...].astype(f32) * scale * gain_two[...]).astype(bf16)

    part = rows // 2
    where = lambda slot, half: rows_two.at[pl.ds(slot * rows + half * part, part), :]
    send(where(0, 1), where(1, 1), bulk.at[1], ag_recv.at[0, 0], side, None, False)
    send(where(0, 0), where(2, 0), bulk.at[1], ag_recv.at[1, 0], across, None, False)
    send(where(0, 0), where(1, 0), bulk.at[1], ag_recv.at[0, 1], side, None, False)
    send(where(0, 1), where(2, 1), bulk.at[1], ag_recv.at[1, 1], across, None, False)
    line_step(2, 1, when=crossed)
    line_step(2, 2, when=when_all(crossed, inner))
    arrive(where(1, 1), ag_recv.at[0, 0])
    send(where(1, 1), where(3, 1), bulk.at[1], ag_recv.at[1, 2], across, None, False)
    arrive(where(2, 0), ag_recv.at[1, 0])
    send(where(2, 0), where(3, 0), bulk.at[1], ag_recv.at[0, 2], side, None, False)
    for rank in far:
        line_step(2, rank, when=inner)
    arrive(where(1, 0), ag_recv.at[0, 1])
    arrive(where(2, 1), ag_recv.at[1, 1])
    arrive(where(3, 0), ag_recv.at[0, 2])
    arrive(where(3, 1), ag_recv.at[1, 2])
    arrive(down_full.at[z * SIDES + c], swap_recv.at[1], crossed)
    for a in (3, 4):
        along(a, z, own=True)
        to_core(a, z)
    lift = 2 * rows
    reach = SIDES * slab
    last = depth - 1
    for rank in range(2, last):
        line_step(2, rank, when=outer)
    for rank in range(last):
        arrive(theirs(2, order[rank]), core_recv.at[2, order[rank]])

    def product(t, here, rank):
        span = pl.ds(pl.multiple_of(order[rank] * reach, reach), reach)
        weight = up_full[pl.ds(order[rank] * SIDES, SIDES), t].reshape(reach, 2 * LANES)
        return jnp.dot(rows_two[here, span], weight, preferred_element_type=f32)

    def partial_tile(t, _):
        for block in range(2):
            here = slice(block * lift, (block + 1) * lift)
            pre = product(t, here, 0)
            for rank in range(1, last):
                pre = pre + product(t, here, rank)
            sums[t, here, :] = pre.astype(bf16)
        return 0

    lax.fori_loop(0, tiles, partial_tile, 0)
    line_step(2, last, when=outer)
    arrive(theirs(2, order[last]), core_recv.at[2, order[last]])

    row_in_seq = lax.rem(lax.broadcasted_iota(jnp.int32, (lift, LANES), 0), SEQ_LEN)

    def raise_tile(t, _):
        cols = pl.ds(pl.multiple_of(t * LANES, LANES), LANES)
        table = param_full[x, 0:ffn_width, pl.ds(pl.multiple_of(chans + t * LANES, LANES), LANES)]
        for block in range(2):
            here = slice(block * lift, (block + 1) * lift)
            pre = sums[t, here, :].astype(f32) + product(t, here, last)
            gate = pre[:, :LANES].astype(bf16).astype(f32)
            value = pre[:, LANES:].astype(bf16).astype(f32)
            conv = gate * table[ffn_width - 1 : ffn_width]
            for back in range(1, ffn_width):
                shifted = shift_rows(gate, back, row_in_seq, 0.0)
                conv = conv + shifted * table[ffn_width - 1 - back : ffn_width - back]
            hidden[here, cols] = (jax.nn.silu(conv) * value).astype(bf16)
        return 0

    lax.fori_loop(0, tiles, raise_tile, 0)

    ffn_own = mix_own

    def cut(ref, h):
        return ref if h is None else ref.at[..., pl.ds(h * thin, thin)]

    def first_leg(j, way, h=None):
        sem = pair_half.at[j % SIDES, way] if h else pair_sem.at[j, way]
        return remote(cut(pair_out.at[j, way], h), cut(pair_in.at[j, way], h), bulk.at[2], sem, (side, across)[way])

    def last_leg(j, way, h=None):
        sem = last_half.at[j % SIDES, way] if h else last_sem.at[j, way]
        return remote(cut(last_out.at[j, way], h), cut(last_in.at[j, way], h), bulk.at[3], sem, (across, side)[way])

    def lower(j, h=None):
        cols = slice(None) if h is None else slice(h * thin, (h + 1) * thin)
        weight = jnp.concatenate([down_full[j, 0], down_full[j, 1]], axis=1) if h is None else down_full[j, h]
        block = jnp.dot(hidden[rows:, :], weight, preferred_element_type=f32)
        for way in range(2):
            for leg, slot in enumerate((way, 2)):
                first = slot * rows + way * part
                pair_out[j, way, leg, :, cols] = block[first : first + part].astype(bf16)
        for way in range(2):
            first_leg(j, way, h).start()
        for way in range(2):
            first = (1 - way) * rows + way * part
            ffn_next[j, way, :, cols] = block[first : first + part]
        ffn_own[j, :, cols] = jnp.dot(hidden[:rows, :], weight, preferred_element_type=f32)

    def pass_on(j, h=None):
        cols = slice(None) if h is None else slice(h * thin, (h + 1) * thin)
        for way in range(2):
            these = slice(way * part, (way + 1) * part)
            first_leg(j, way, h).wait_recv()
            last_out[j, way, :, cols] = (
                ffn_next[j, way, :, cols] + pair_in[j, way, 1, :, cols].astype(f32)
            ).astype(bf16)
            last_leg(j, way, h).start()
            ffn_own[j, these, cols] = ffn_own[j, these, cols] + pair_in[j, way, 0, :, cols].astype(f32)

    def store(j):
        lanes = pl.ds(pl.multiple_of(j * slab, slab), slab)
        return pltpu.make_async_copy(made.at[:, lanes], result.at[:, lanes], bulk.at[4])

    def finish(j, halves=(None,)):
        lanes = pl.ds(pl.multiple_of(j * slab, slab), slab)
        for way in range(2):
            for h in halves:
                last_leg(j, way, h).wait_recv()
        for way in range(2):
            these = slice(way * part, (way + 1) * part)
            summed = ffn_own[j, these, :] + last_in[j, way].astype(f32)
            made[these, lanes] = (middle[these, lanes].astype(f32) + summed).astype(bf16)
        store(j).start()

    def slab_of(rank, turn):
        return order[rank] * SIDES + (c, 1 - c)[turn]

    def both(act, rank):
        for turn in range(SIDES):
            act(slab_of(rank, turn))

    for rank in range(last):
        for a in (3, 4):
            if rank == 1:
                line_step(a, 1)
                if 2 < last:
                    line_step(a, 2, when=inner)
            elif rank == 2:
                line_step(a, 2, when=outer)
            elif rank:
                line_step(a, rank)
        lower(slab_of(rank, 0))
        for a in (3, 4):
            arrive(theirs(a, order[rank]), core_recv.at[a, order[rank]])
        lower(slab_of(rank, 1))
        if rank:
            both(pass_on, rank - 1)
    both(finish, 0)
    for h in range(2):
        with jax.named_scope("lstep"):
            line_step(3 + h, last)
        with jax.named_scope("ldot"):
            lower(slab_of(last, 0), h)
        with jax.named_scope("lcore"):
            arrive(theirs(3 + h, order[last]), core_recv.at[3 + h, order[last]])
        with jax.named_scope("ldot"):
            lower(slab_of(last, 1), h)
        with jax.named_scope("lpass"):
            if h == 0:
                both(pass_on, last - 1)
            else:
                for rank in range(1, last):
                    both(finish, rank)
    for h in range(2):
        for turn in range(SIDES):
            pass_on(slab_of(last, turn), h)
    for turn in range(SIDES):
        finish(slab_of(last, turn), (0, 1))

    for when, make in flights:
        if when is None:
            make().wait_send()
        else:
            pl.when(when)(lambda make=make: make().wait_send())

    @pl.when(crossed)
    def _():
        gone(mine(2, z), swap_send.at[0])
        gone(down_full.at[z * SIDES + x], swap_send.at[1])

    mine_out = pl.ds(pl.multiple_of(c * chans, chans), chans)
    gone(in_full.at[c, pl.ds(0, depth * slab), :], side_send.at[0])
    gone(out_full.at[pl.ds(0, depth), mine_out, :], side_send.at[1])
    gone(in_full.at[c], core_send.at[0])
    gone(out_full.at[:, mine_out, :], core_send.at[1])
    gone(up_full.at[pl.ds(0, depth)], core_send.at[2])
    for h in range(2):
        gone(down_full.at[pl.ds(0, depth), h], core_send.at[3 + h])
    gone(mix_send, bulk.at[0])
    gone(rows_two.at[pl.ds(0, 3 * rows), :], bulk.at[1])
    gone(pair_out, bulk.at[2])
    gone(last_out, bulk.at[3])
    pltpu.make_async_copy(made, result, bulk.at[4]).wait()


def resident(
    n_fs, n_tp, resid, mix_gain, in_weight, conv_taps, recur_gate_w, input_gate_w, decay_rate,
    out_weight, mlp_gain, up_gate_w, up_val_w, ffn_taps, down_weight,
):
    depth = n_fs // SIDES
    rows, width = resid.shape
    slab, chans = in_weight.shape
    units = up_gate_w.shape[1]
    slabs = width // slab
    tiles = units // LANES
    bf16, f32 = jnp.bfloat16, jnp.float32
    vmem = pl.BlockSpec(memory_space=pltpu.VMEM)
    hbm = pl.BlockSpec(memory_space=pl.ANY)
    dma = pltpu.SemaphoreType.DMA
    return pl.pallas_call(
        functools.partial(resident_kernel, depth),
        out_shape=jax.ShapeDtypeStruct((rows, width), bf16),
        in_specs=[hbm] + [vmem] * 7 + [hbm] * 5,
        out_specs=hbm,
        scratch_shapes=[
            pltpu.VMEM((rows, width), bf16),
            pltpu.VMEM((CORES, width, chans), bf16),
            pltpu.VMEM((slabs, CORES * chans, slab), bf16),
            pltpu.VMEM((slabs, tiles, slab, 2 * LANES), bf16),
            pltpu.VMEM((slabs, 2, units, slab // 2), bf16),
            pltpu.VMEM((CORES, 8, chans + units), f32),
            pltpu.VMEM((CORES, chans // LANES, LANES, 2 * LANES), bf16),
            pltpu.VMEM((2 * rows, width), bf16),
            pltpu.VMEM((2 * rows, CORES * chans), bf16),
            pltpu.VMEM((2 * rows, CORES * chans), bf16),
            pltpu.VMEM((slabs, rows, slab), f32),
            pltpu.VMEM((slabs, rows, slab), bf16),
            pltpu.VMEM((slabs, rows, slab), bf16),
            pltpu.VMEM((rows, width), bf16),
            pltpu.VMEM((4 * rows, width), bf16),
            pltpu.VMEM((4 * rows, units), bf16),
            pltpu.VMEM((tiles, 4 * rows, 2 * LANES), bf16),
            pltpu.VMEM((slabs, 2, rows // 2, slab), f32),
            pltpu.VMEM((slabs, 2, 2, rows // 2, slab), bf16),
            pltpu.VMEM((slabs, 2, 2, rows // 2, slab), bf16),
            pltpu.VMEM((slabs, 2, rows // 2, slab), bf16),
            pltpu.VMEM((slabs, 2, rows // 2, slab), bf16),
            pltpu.VMEM((rows, width), bf16),
            dma((6,)),
            dma((5, depth)), dma((5,)), dma((5, depth)),
            dma((2,)), dma((2, depth)),
            dma((5,)), dma((5, depth)),
            dma((2,)), dma((2,)),
            dma((2,)), dma((2,)),
            dma((2,)),
            dma((slabs,)),
            dma((2, 3)),
            dma((slabs, 2)), dma((2, 2)),
            dma((slabs, 2)), dma((2, 2)),
            dma((5,)),
        ],
        compiler_params=pltpu.CompilerParams(
            collective_id=0, has_side_effects=True, vmem_limit_bytes=VMEM_BYTES
        ),
    )(
        resid, mix_gain.reshape(1, -1), mlp_gain.reshape(1, -1), conv_taps, decay_rate.reshape(1, -1),
        ffn_taps, recur_gate_w, input_gate_w, in_weight, out_weight, up_gate_w, up_val_w, down_weight,
    )


def solution(mesh):
    in_specs = (
        P(("fs", "tp"), None),
        P(),
        P("fs", "tp"),
        P(None, "tp"),
        P("tp", None, None),
        P("tp", None, None),
        P("tp"),
        P("tp", "fs"),
        P(),
        P("fs", "tp"),
        P("fs", "tp"),
        P(None, "tp"),
        P("tp", "fs"),
    )
    out_specs = P(("fs", "tp"), None)
    n_fs, n_tp = mesh.shape["fs"], mesh.shape["tp"]
    body = functools.partial(resident if fits(n_fs, n_tp) else shards, n_fs, n_tp)
    return jax.shard_map(body, mesh=mesh, in_specs=in_specs, out_specs=out_specs, check_vma=False)
```

```python
import functools

import jax
import jax.numpy as jnp
from jax import lax
from jax.experimental import pallas as pl
from jax.experimental.pallas import tpu as pltpu
from jax.sharding import PartitionSpec as P

GATE_BLOCK = 64
SEQ_LEN = 128
LANES = 128
CORES = 2


def rms_scale(rows_in, gain_vec):
    wide = rows_in.astype(jnp.float32)
    return wide * lax.rsqrt(jnp.mean(wide * wide, axis=-1, keepdims=True) + 1e-06) * gain_vec


def causal_taps(values, tap_weights):
    width = tap_weights.shape[0]
    length = values.shape[1]
    padded = jnp.pad(values, ((0, 0), (width - 1, 0), (0, 0)))
    summed = jnp.zeros_like(values)
    for tap_index in range(width):
        summed = summed + padded[:, tap_index : tap_index + length] * tap_weights[tap_index]
    return summed


def negative_expm1(arg):
    series = jnp.ones_like(arg)
    for order in range(8, 1, -1):
        series = 1.0 + arg * (1.0 / order) * series
    return jnp.where(arg > -0.5, -arg * series, 1.0 - jnp.exp(arg))


def shift_rows(values, distance, rows, fill):
    return jnp.where(rows >= distance, pltpu.roll(values, distance, 0), fill)


def recurrence_kernel(projected_ref, taps_ref, gates_ref, rate_ref, out_ref):
    width = taps_ref.shape[0]
    rows = lax.broadcasted_iota(jnp.int32, (SEQ_LEN, LANES), 0)
    for chunk in range(projected_ref.shape[1] // LANES):
        cols = slice(chunk * LANES, (chunk + 1) * LANES)
        values = projected_ref[:, cols].astype(jnp.float32)
        conv = values * taps_ref[width - 1 : width, cols]
        for back in range(1, width):
            tap = taps_ref[width - 1 - back : width - back, cols]
            conv = conv + shift_rows(values, back, rows, 0.0) * tap
        gates = jax.nn.sigmoid(
            jnp.dot(
                conv.astype(jnp.bfloat16), gates_ref[chunk], preferred_element_type=jnp.float32
            )
        )
        rgate = gates[:, :LANES]
        igate = gates[:, LANES:]
        logdecay = -8.0 * rgate * rate_ref[:, cols]
        decay = jnp.exp(logdecay)
        state = jnp.sqrt(negative_expm1(2.0 * logdecay)) * (igate * conv)
        distance = 1
        while distance < SEQ_LEN:
            state = state + decay * shift_rows(state, distance, rows, 0.0)
            if 2 * distance < SEQ_LEN:
                decay = decay * shift_rows(decay, distance, rows, 1.0)
            distance *= 2
        out_ref[:, cols] = state.astype(jnp.bfloat16)


def pair_blocks(blocks):
    pairs = blocks.reshape(-1, 2, GATE_BLOCK, GATE_BLOCK)
    blank = jnp.zeros_like(pairs[:, 0])
    upper = jnp.concatenate([pairs[:, 0], blank], axis=2)
    lower = jnp.concatenate([blank, pairs[:, 1]], axis=2)
    return jnp.concatenate([upper, lower], axis=1)


def recurrence(projected, conv_taps, gates, decay_rate):
    count, channels = projected.shape
    whole = lambda shape: pl.BlockSpec(shape, lambda seq: (0,) * len(shape))
    return pl.pallas_call(
        recurrence_kernel,
        grid=(count // SEQ_LEN,),
        in_specs=[
            pl.BlockSpec((SEQ_LEN, channels), lambda seq: (seq, 0)),
            whole(conv_taps.shape),
            whole(gates.shape),
            whole((1, channels)),
        ],
        out_specs=pl.BlockSpec((SEQ_LEN, channels), lambda seq: (seq, 0)),
        out_shape=jax.ShapeDtypeStruct(projected.shape, jnp.bfloat16),
        cost_estimate=pl.CostEstimate(
            flops=count * channels * 600, bytes_accessed=count * channels * 4,
            transcendentals=count * channels * 6,
        ),
    )(projected, conv_taps, gates, decay_rate.reshape(1, channels))


def gather_groups(block, n_tp):
    sides = n_tp // CORES
    swap = [(i, i ^ 1) for i in range(n_tp)]
    groups = []
    for distance in range(sides):
        mine = block
        if distance:
            back = [
                (i, ((i // CORES - distance) % sides) * CORES + i % CORES) for i in range(n_tp)
            ]
            mine = lax.ppermute(block, "tp", back)
        groups.append(jnp.concatenate([mine, lax.ppermute(mine, "tp", swap)], axis=0))
    return groups


def scatter_sum(partial_of, n_tp):
    sides = n_tp // CORES
    swap = [(i, i ^ 1) for i in range(n_tp)]
    total = 0.0
    for distance in reversed(range(sides)):
        partial = partial_of(distance)
        half = partial.shape[0] // 2
        other = lax.ppermute(partial[half:], "tp", swap)
        pair = partial[:half].astype(jnp.float32) + other.astype(jnp.float32)
        if distance:
            ahead = [
                (i, ((i // CORES + distance) % sides) * CORES + i % CORES) for i in range(n_tp)
            ]
            pair = lax.ppermute(pair.astype(jnp.bfloat16), "tp", ahead).astype(jnp.float32)
        total = total + pair
    return total


def gather_weight(block, n_fs, n_tp):
    inner = n_tp // CORES if n_fs % (n_tp // CORES) == 0 else 1
    outer = n_fs // inner
    me = lax.axis_index("fs")
    parts = [block]
    for distance in range(1, outer):
        back = [(i, (i - distance * inner) % n_fs) for i in range(n_fs)]
        parts.append(lax.ppermute(block, "fs", back))
    start = lax.rem(outer - me // inner, outer)
    column = lax.dynamic_slice_in_dim(jnp.stack(parts + parts[:-1]), start, outer, 0)
    parts = [column]
    for distance in range(1, inner):
        back = [(i, i // inner * inner + (i - distance) % inner) for i in range(n_fs)]
        parts.append(lax.ppermute(column, "fs", back))
    start = lax.rem(inner - lax.rem(me, inner), inner)
    stacked = jnp.stack(parts + parts[:-1], axis=1)
    stacked = lax.dynamic_slice_in_dim(stacked, start, inner, 1)
    return stacked.reshape((n_fs,) + block.shape)


def side_by_side(stacked):
    return jnp.transpose(stacked, (1, 0, 2)).reshape(stacked.shape[1], -1)


def dot(left, right):
    return jnp.dot(left, right, preferred_element_type=jnp.float32).astype(jnp.bfloat16)


def shards(
    n_fs,
    n_tp,
    resid,
    mix_gain,
    in_weight,
    conv_taps,
    recur_gate_w,
    input_gate_w,
    decay_rate,
    out_weight,
    mlp_gain,
    up_gate_w,
    up_val_w,
    ffn_taps,
    down_weight,
):
    gate_full = lax.all_gather(up_gate_w, "fs", axis=0, tiled=True)
    val_full = lax.all_gather(up_val_w, "fs", axis=0, tiled=True)
    cut = down_weight.shape[0] - down_weight.shape[0] // (2 * LANES) * LANES
    down_head = lax.all_gather(down_weight[:cut], "fs", axis=1, tiled=True)
    in_full = gather_weight(in_weight, n_fs, n_tp).reshape(-1, in_weight.shape[1])
    out_full = side_by_side(gather_weight(out_weight, n_fs, n_tp))
    later = lax.optimization_barrier((down_weight[cut:], in_full))[0]
    down_tail = side_by_side(gather_weight(later, n_fs, n_tp))
    gates = jnp.concatenate([pair_blocks(recur_gate_w), pair_blocks(input_gate_w)], axis=2)

    normed = rms_scale(resid, mix_gain).astype(jnp.bfloat16)
    recurred = [
        recurrence(dot(rows, in_full), conv_taps, gates, decay_rate)
        for rows in gather_groups(normed, n_tp)
    ]
    mixed_sum = scatter_sum(lambda distance: dot(recurred[distance], out_full), n_tp)
    middle = (resid.astype(jnp.float32) + mixed_sum).astype(jnp.bfloat16)
    normed_two = rms_scale(middle, mlp_gain).astype(jnp.bfloat16)

    hidden = []
    for rows in gather_groups(normed_two, n_tp):
        gate_pre = dot(rows, gate_full)
        value_pre = dot(rows, val_full)
        seqs = gate_pre.shape[0] // SEQ_LEN
        gate_conv = causal_taps(
            gate_pre.astype(jnp.float32).reshape(seqs, SEQ_LEN, -1), ffn_taps
        ).reshape(gate_pre.shape)
        hidden.append((jax.nn.silu(gate_conv) * value_pre.astype(jnp.float32)).astype(jnp.bfloat16))
    tails = [
        jnp.dot(rows[:, cut:], down_tail, preferred_element_type=jnp.float32) for rows in hidden
    ]

    def down_partial(distance):
        head = jnp.dot(hidden[distance][:, :cut], down_head, preferred_element_type=jnp.float32)
        return (head + tails[distance]).astype(jnp.bfloat16)

    ffn_sum = scatter_sum(down_partial, n_tp)
    return (middle.astype(jnp.float32) + ffn_sum).astype(jnp.bfloat16)


MESH = pl.DeviceIdType.MESH
SIDES = 2
VMEM_BYTES = 66_000_000


def fits(n_fs, n_tp):
    return n_tp == SIDES * CORES and n_fs == SIDES * 2 * SIDES


def line_order(depth, z):
    ranks = []
    for here in range(depth):
        up_first = here < depth / 2
        others = [p for p in range(depth) if p != here]
        others.sort(key=lambda p: (abs(p - here), (p < here) == up_first))
        ranks.append([here] + others)
    order = []
    for rank in range(depth):
        place = jnp.int32(0)
        for here in range(depth):
            place = jnp.where(z == here, ranks[here][rank], place)
        order.append(place)
    return order


def resident_kernel(
    depth,
    resid_in, gain_one_in, gain_two_in, conv_taps_in, decay_rate_in, ffn_taps_in, recur_gate_in, input_gate_in,
    in_w, out_w, gate_w, val_w, down_w,
    result,
    gain_one, gain_two, conv_taps, decay_rate, ffn_taps, recur_gate, input_gate, table_sem,
    resid, in_full, out_full, up_full, down_full, param_full, gate_full,
    normed, proj, recurred, mix_own, mix_send, mix_recv, middle, rows_two, hidden,
    sums, ffn_next, pair_out, pair_in, last_out, last_in, made,
    local_sem, line_send, line_twin, line_recv, side_send, side_recv, core_send, core_recv,
    swap_send, swap_recv, small_send, small_recv, row_sems, mix_recv_sem, ag_recv,
    pair_sem, pair_half, last_sem, last_half, bulk, far_send, far_recv, far_core,
):
    f32, bf16 = jnp.float32, jnp.bfloat16
    fs, tp = lax.axis_index("fs"), lax.axis_index("tp")
    z, x = fs // SIDES, lax.rem(fs, SIDES)
    y, c = tp // CORES, lax.rem(tp, CORES)
    rows, width = resid.shape
    slab, chans = in_w.shape
    taps, ffn_width = conv_taps.shape[0], ffn_taps.shape[0]
    tiles = gate_w.shape[1] // LANES
    slabs = width // slab
    n_seq = rows // SEQ_LEN
    order = line_order(depth, z)
    straight, crossed = x == c, x != c
    has_up, has_down = z < depth - 1, z > 0
    inner = jnp.logical_and(has_up, has_down)
    outer = jnp.logical_not(inner)
    near, far = range(1, min(3, depth)), range(3, depth)

    at = lambda zz, xx, yy, cc: (zz * SIDES + xx, yy * CORES + cc)
    up, down = at(z + 1, x, y, c), at(z - 1, x, y, c)
    side, core, swap = at(z, 1 - x, y, c), at(z, x, y, 1 - c), at(z, c, y, x)
    across = at(z, x, 1 - y, c)

    barrier = pltpu.get_barrier_semaphore()
    greet = lambda dev: pl.semaphore_signal(barrier, inc=1, device_id=dev, device_id_type=MESH)
    for dev in (side, core, across):
        greet(dev)
    for when, dev in ((has_up, up), (has_down, down), (crossed, swap)):
        pl.when(when)(functools.partial(greet, dev))
    one = lambda when: when.astype(jnp.int32)
    pl.semaphore_wait(barrier, 3 + one(has_up) + one(has_down) + one(crossed))

    flights = []

    def when_all(*conds):
        conds = [cond for cond in conds if cond is not None]
        return functools.reduce(jnp.logical_and, conds) if conds else None

    def remote(src, dst, ss, rs, dev):
        return pltpu.make_async_remote_copy(
            src_ref=src, dst_ref=dst, send_sem=ss, recv_sem=rs, device_id=dev, device_id_type=MESH
        )

    def send(src, dst, ss, rs, dev, when=None, alone=True):
        make = functools.partial(remote, src, dst, ss, rs, dev)
        if when is None:
            make().start()
        else:
            pl.when(when)(lambda: make().start())
        if alone:
            flights.append((when, make))

    def gone(whole, ss):
        remote(whole, whole, ss, ss, core).wait_send()

    def arrive(dst, rs, when=None):
        wait = lambda: remote(dst, dst, rs, rs, core).wait_recv()
        if when is None:
            wait()
        else:
            pl.when(when)(wait)

    def row_slab(zz, xx):
        return pl.ds(pl.multiple_of((zz * SIDES + xx) * slab, slab), slab)

    def place(a, zz, xx, cc):
        if a == 0:
            return in_full.at[cc, row_slab(zz, xx), :]
        if a == 1:
            return out_full.at[zz * SIDES + xx, pl.ds(pl.multiple_of(cc * chans, chans), chans), :]
        if a == 2:
            return up_full.at[zz * SIDES + xx]
        return down_full.at[zz * SIDES + xx, a - 3]

    def mine(a, zz):
        return place(a, zz, x, c) if a < 2 else place(a, zz, c, c)

    def theirs(a, zz):
        return place(a, zz, x, 1 - c) if a < 2 else place(a, zz, 1 - c, c)

    def along(a, zz, src=None, when=None, own=False):
        dst = mine(a, zz)
        src = dst if src is None else src
        ups = has_up if own else jnp.logical_and(zz < z, has_up)
        downs = has_down if own else jnp.logical_and(zz > z, has_down)
        twin = line_twin.at[a] if own else line_send.at[a, zz]
        send(src, dst, line_send.at[a, zz], line_recv.at[a, zz], up, when_all(ups, when))
        send(src, dst, twin, line_recv.at[a, zz], down, when_all(downs, when))

    def to_side(a, zz, src=None, when=None):
        dst = mine(a, zz)
        send(dst if src is None else src, dst, side_send.at[a], side_recv.at[a, zz], side, when, False)

    def core_sem(a, zz):
        return core_recv.at[a, 0] if a == 0 else core_recv.at[a, zz]

    def to_core(a, zz, src=None, when=None):
        dst = mine(a, zz)
        send(dst if src is None else src, dst, core_send.at[a], core_sem(a, zz), core, when, False)

    def line_step(a, rank, when=None):
        if rank >= depth:
            return
        zz = order[rank]
        arrive(mine(a, zz), line_recv.at[a, zz], when)
        along(a, zz, when=when)
        if a < 2:
            to_side(a, zz, when=when_all(when, (None, crossed)[a]))
        to_core(a, zz, when=when)

    def side_step(a, rank):
        if rank >= depth:
            return
        zz = order[rank]
        dst = place(a, zz, 1 - x, c)
        arrive(dst, side_recv.at[a, zz])
        send(dst, dst, core_send.at[a], core_sem(a, zz), core, None, False)

    in_copy = pltpu.make_async_copy(in_w, mine(0, z), local_sem.at[0])
    out_copy = pltpu.make_async_copy(out_w, mine(1, z), local_sem.at[1])
    up_copy = pltpu.make_async_copy(mine(2, z), mine(2, z), local_sem.at[2])
    thin = slab // 2
    down_part = lambda h: down_w.at[:, pl.ds(h * thin, thin)]
    down_copies = [pltpu.make_async_copy(down_part(h), mine(3 + h, z), local_sem.at[3 + h]) for h in range(2)]
    resid_copy = pltpu.make_async_copy(resid_in, resid, local_sem.at[5])

    def up_parts():
        for tile in range(tiles):
            for half, weight in enumerate((gate_w, val_w)):
                yield (
                    weight.at[:, pl.ds(tile * LANES, LANES)],
                    up_full.at[z * SIDES + x, tile, :, pl.ds(half * LANES, LANES)],
                )

    resid_copy.start()
    along(0, z, src=in_w, own=True)
    to_side(0, z, src=in_w)
    to_core(0, z, src=in_w)
    in_copy.start()
    out_copy.start()

    table_copies = [
        pltpu.make_async_copy(src, dst, table_sem.at[i])
        for i, (src, dst) in enumerate(
            (
                (gain_one_in, gain_one), (gain_two_in, gain_two), (conv_taps_in, conv_taps),
                (decay_rate_in, decay_rate), (ffn_taps_in, ffn_taps), (recur_gate_in, recur_gate),
                (input_gate_in, input_gate),
            )
        )
    ]
    for copy in table_copies:
        copy.start()
    for copy in table_copies:
        copy.wait()
    param_full[c, 0:taps, 0:chans] = conv_taps[...]
    param_full[c, taps : taps + 1, 0:chans] = decay_rate[...]
    param_full[c, 0:ffn_width, chans:] = ffn_taps[...]
    spot = lambda axis: lax.broadcasted_iota(jnp.int32, (GATE_BLOCK, LANES), axis)
    for half in range(LANES // GATE_BLOCK):
        spread = (spot(0) + half * GATE_BLOCK == spot(1)).astype(f32).astype(bf16)
        for kind, blocks in enumerate((recur_gate, input_gate)):
            for pair in range(chans // LANES):
                gate_full[
                    c, pair, half * GATE_BLOCK : (half + 1) * GATE_BLOCK, kind * LANES : (kind + 1) * LANES
                ] = jnp.dot(blocks[2 * pair + half], spread, preferred_element_type=f32).astype(bf16)
    resid_copy.wait()
    wide = resid[...].astype(f32)
    scale = lax.rsqrt(jnp.mean(wide * wide, axis=-1, keepdims=True) + 1e-06)
    normed[0:rows, :] = (wide * scale * gain_one[...]).astype(bf16)
    for i, full in enumerate((param_full, gate_full)):
        send(full.at[c], full.at[c], small_send.at[i], small_recv.at[i], core)
    send(normed.at[pl.ds(0, rows), :], normed.at[pl.ds(rows, rows), :], row_sems.at[0], row_sems.at[1], across)

    @pl.when(straight)
    def _():
        for src, dst in up_parts():
            pltpu.make_async_copy(src, dst, local_sem.at[2]).start()
        for copy in down_copies:
            copy.start()

    for rank in near:
        line_step(0, rank)
    along(1, z, src=out_w, own=True)
    to_core(1, z, src=out_w)
    side_step(0, 0)
    side_step(0, 1)

    def swap_some(parts):
        @pl.when(crossed)
        def _():
            for src, dst in parts:
                remote(src, dst, swap_send.at[0], swap_recv.at[0], swap).start()

    parts = list(up_parts())
    swap_some(parts[:tiles])
    for rank in far:
        line_step(0, rank)
    swap_some(parts[tiles:])
    to_side(1, z, src=out_w, when=crossed)
    side_step(0, 2)
    for rank in near:
        line_step(1, rank)

    def out_and_up(when):
        for rank in far:
            line_step(1, rank, when=when)
        ready = jnp.logical_and(straight, when)

        @pl.when(ready)
        def _():
            up_copy.wait()
            for copy in down_copies:
                copy.wait()

        along(2, z, when=ready, own=True)
        to_core(2, z, when=ready)

    out_and_up(inner)
    for rank in far:
        side_step(0, rank)
    in_copy.wait()
    out_copy.wait()
    for i, full in enumerate((param_full, gate_full)):
        arrive(full.at[1 - c], small_recv.at[i])
    arrive(in_full.at[1 - c], core_recv.at[0, 0])
    arrive(normed.at[pl.ds(rows, rows), :], row_sems.at[1])

    wide_n = 2 * LANES
    per = chans // wide_n

    def project(i, _):
        cc, h = i // per, lax.rem(i, per)
        lanes = pl.ds(pl.multiple_of(h * wide_n, wide_n), wide_n)
        to = pl.ds(pl.multiple_of(i * wide_n, wide_n), wide_n)
        proj[:, to] = jnp.dot(normed[...], in_full[cc, :, lanes], preferred_element_type=f32).astype(bf16)
        return 0

    lax.fori_loop(0, CORES * per, project, 0)

    to_side(1, z, src=out_w, when=straight)
    for rank in near:
        to_side(1, order[rank], when=straight)
    out_and_up(outer)
    for rank in far:
        to_side(1, order[rank], when=straight)
    for h in range(2):
        send(down_part(h), place(3 + h, z, x, c), swap_send.at[1], swap_recv.at[1], swap, crossed, False)

    position = lax.broadcasted_iota(jnp.int32, (SEQ_LEN, LANES), 0)
    chan_tiles = chans // LANES

    def recur(seq):
        where = pl.ds(seq * SEQ_LEN, SEQ_LEN)

        def tile_step(i, _):
            cc, u = i // chan_tiles, lax.rem(i, chan_tiles)
            cols = pl.ds(pl.multiple_of(u * LANES, LANES), LANES)
            to = pl.ds(pl.multiple_of(i * LANES, LANES), LANES)
            values = proj[where, to].astype(f32)
            table = param_full[cc, 0 : taps + 1, cols]
            conv = values * table[taps - 1 : taps]
            for back in range(1, taps):
                conv = conv + shift_rows(values, back, position, 0.0) * table[taps - 1 - back : taps - back]
            both = jax.nn.sigmoid(jnp.dot(conv.astype(bf16), gate_full[cc, u], preferred_element_type=f32))
            logdecay = -8.0 * both[:, :LANES] * table[taps : taps + 1]
            decay = jnp.exp(logdecay)
            state = jnp.sqrt(negative_expm1(2.0 * logdecay)) * (both[:, LANES:] * conv)
            distance = 1
            while distance < SEQ_LEN:
                state = state + decay * shift_rows(state, distance, position, 0.0)
                if 2 * distance < SEQ_LEN:
                    decay = decay * shift_rows(decay, distance, position, 1.0)
                distance *= 2
            recurred[where, to] = state.astype(bf16)
            return 0

        lax.fori_loop(0, CORES * chan_tiles, tile_step, 0)

    for seq in reversed(range(2 * n_seq)):
        recur(seq)
        if seq < 2:
            side_step(1, 1 - seq)

    arrive(mine(2, z), swap_recv.at[0], crossed)
    along(2, z, when=crossed, own=True)
    to_core(2, z, when=crossed)

    def mix_copy(j):
        return remote(mix_send.at[j], mix_recv.at[j], bulk.at[0], mix_recv_sem.at[j], across)

    for rank in range(depth):
        zz = order[rank]
        if rank >= 2:
            side_step(1, rank)
        theirs_out = pl.ds(pl.multiple_of((1 - c) * chans, chans), chans)
        arrive(out_full.at[pl.ds(zz * SIDES, SIDES), theirs_out, :], core_recv.at[1, zz])

        def mix(s, _):
            j = zz * SIDES + s
            both = jnp.dot(recurred[...], out_full[j], preferred_element_type=f32)
            mix_send[j] = both[rows:].astype(bf16)
            mix_copy(j).start()
            mix_own[j] = both[:rows]
            return 0

        lax.fori_loop(0, SIDES, mix, 0)
        if rank == 1:
            with jax.named_scope("up1_straight"):
                line_step(2, 1, when=straight)
                line_step(2, 2, when=when_all(straight, inner))

    total = jnp.zeros((rows, 1), f32)
    for j in range(slabs):
        mix_copy(j).wait_recv()
        lanes = slice(j * slab, (j + 1) * slab)
        value = (resid[:, lanes].astype(f32) + (mix_own[j] + mix_recv[j].astype(f32))).astype(bf16)
        middle[:, lanes] = value
        value = value.astype(f32)
        total = total + jnp.sum(value * value, axis=-1, keepdims=True)
    scale = lax.rsqrt(total * (1.0 / width) + 1e-06)
    rows_two[0:rows, :] = (middle[...].astype(f32) * scale * gain_two[...]).astype(bf16)

    part = rows // 2
    where = lambda slot, half: rows_two.at[pl.ds(slot * rows + half * part, part), :]
    send(where(0, 1), where(1, 1), bulk.at[1], ag_recv.at[0, 0], side, None, False)
    send(where(0, 0), where(2, 0), bulk.at[1], ag_recv.at[1, 0], across, None, False)
    send(where(0, 0), where(1, 0), bulk.at[1], ag_recv.at[0, 1], side, None, False)
    send(where(0, 1), where(2, 1), bulk.at[1], ag_recv.at[1, 1], across, None, False)
    line_step(2, 1, when=crossed)
    line_step(2, 2, when=when_all(crossed, inner))
    arrive(where(1, 1), ag_recv.at[0, 0])
    send(where(1, 1), where(3, 1), bulk.at[1], ag_recv.at[1, 2], across, None, False)
    arrive(where(2, 0), ag_recv.at[1, 0])
    send(where(2, 0), where(3, 0), bulk.at[1], ag_recv.at[0, 2], side, None, False)
    last = depth - 1
    cut_at = tiles // 2 + 1
    far_tiles = ((0, cut_at), (cut_at, tiles))
    far_piece = lambda ref, k: ref.at[pl.ds(far_tiles[k][0], far_tiles[k][1] - far_tiles[k][0])]
    zz = order[last]
    arrive(mine(2, zz), line_recv.at[2, zz], inner)
    for k in range(2):
        piece = far_piece(mine(2, zz), k)
        send(piece, piece, far_send.at[k], far_recv.at[k], up, when_all(inner, zz < z))
        send(piece, piece, far_send.at[k], far_recv.at[k], down, when_all(inner, zz > z))
    for k in range(2):
        piece = far_piece(mine(2, zz), k)
        send(piece, piece, core_send.at[2], far_core.at[k], core, inner, False)
    arrive(where(1, 0), ag_recv.at[0, 1])
    arrive(where(2, 1), ag_recv.at[1, 1])
    arrive(where(3, 0), ag_recv.at[0, 2])
    arrive(where(3, 1), ag_recv.at[1, 2])
    arrive(down_full.at[z * SIDES + c], swap_recv.at[1], crossed)
    for a in (3, 4):
        along(a, z, own=True)
        to_core(a, z)
    lift = 2 * rows
    reach = SIDES * slab
    for rank in range(2, last):
        line_step(2, rank, when=outer)
    for rank in range(last):
        arrive(theirs(2, order[rank]), core_recv.at[2, order[rank]])

    def product(t, here, rank):
        span = pl.ds(pl.multiple_of(order[rank] * reach, reach), reach)
        weight = up_full[pl.ds(order[rank] * SIDES, SIDES), t].reshape(reach, 2 * LANES)
        return jnp.dot(rows_two[here, span], weight, preferred_element_type=f32)

    def partial_tile(t, _):
        for block in range(2):
            here = slice(block * lift, (block + 1) * lift)
            pre = product(t, here, 0)
            for rank in range(1, last):
                pre = pre + product(t, here, rank)
            sums[t, here, :] = pre.astype(bf16)
        return 0

    lax.fori_loop(0, tiles, partial_tile, 0)
    row_in_seq = lax.rem(lax.broadcasted_iota(jnp.int32, (lift, LANES), 0), SEQ_LEN)

    def raise_tile(t, _):
        cols = pl.ds(pl.multiple_of(t * LANES, LANES), LANES)
        table = param_full[x, 0:ffn_width, pl.ds(pl.multiple_of(chans + t * LANES, LANES), LANES)]
        for block in range(2):
            here = slice(block * lift, (block + 1) * lift)
            pre = sums[t, here, :].astype(f32) + product(t, here, last)
            gate = pre[:, :LANES].astype(bf16).astype(f32)
            value = pre[:, LANES:].astype(bf16).astype(f32)
            conv = gate * table[ffn_width - 1 : ffn_width]
            for back in range(1, ffn_width):
                shifted = shift_rows(gate, back, row_in_seq, 0.0)
                conv = conv + shifted * table[ffn_width - 1 - back : ffn_width - back]
            hidden[here, cols] = (jax.nn.silu(conv) * value).astype(bf16)
        return 0

    for k in range(2):
        with jax.named_scope("up_last"):
            piece = far_piece(mine(2, order[last]), k)
            arrive(piece, far_recv.at[k], outer)
            send(piece, piece, core_send.at[2], far_core.at[k], core, outer, False)
            arrive(far_piece(theirs(2, order[last]), k), far_core.at[k])
        lax.fori_loop(*far_tiles[k], raise_tile, 0)

    ffn_own = mix_own

    def cut(ref, h):
        return ref if h is None else ref.at[h]

    def columns(h):
        return [(hh, slice(hh * thin, (hh + 1) * thin)) for hh in ((0, 1) if h is None else (h,))]

    def first_leg(j, way, h=None):
        sem = pair_half.at[j % SIDES, way] if h else pair_sem.at[j, way]
        return remote(cut(pair_out.at[j, way], h), cut(pair_in.at[j, way], h), bulk.at[2], sem, (side, across)[way])

    def last_leg(j, way, h=None):
        sem = last_half.at[j % SIDES, way] if h else last_sem.at[j, way]
        return remote(cut(last_out.at[j, way], h), cut(last_in.at[j, way], h), bulk.at[3], sem, (across, side)[way])

    def lower(j, h=None, split=False):
        cols = slice(None) if h is None else slice(h * thin, (h + 1) * thin)
        weight = jnp.concatenate([down_full[j, 0], down_full[j, 1]], axis=1) if h is None else down_full[j, h]
        block = jnp.dot(hidden[rows:, :], weight, preferred_element_type=f32)
        for way in range(2):
            for leg, slot in enumerate((way, 2)):
                first = slot * rows + way * part
                for hh, lanes in columns(h):
                    value = block[first : first + part, lanes if h is None else slice(None)]
                    pair_out[j, way, hh, leg] = value.astype(bf16)
        for part_h in (0, 1) if split else (h,):
            for way in range(2):
                first_leg(j, way, part_h).start()
        for way in range(2):
            first = (1 - way) * rows + way * part
            ffn_next[j, way, :, cols] = block[first : first + part]
        ffn_own[j, :, cols] = jnp.dot(hidden[:rows, :], weight, preferred_element_type=f32)

    def pass_on(j, h=None, ways=(0, 1)):
        for way in ways:
            these = slice(way * part, (way + 1) * part)
            first_leg(j, way, h).wait_recv()
            for hh, cols in columns(h):
                last_out[j, way, hh] = (
                    ffn_next[j, way, :, cols] + pair_in[j, way, hh, 1].astype(f32)
                ).astype(bf16)
            last_leg(j, way, h).start()
            for hh, cols in columns(h):
                ffn_own[j, these, cols] = ffn_own[j, these, cols] + pair_in[j, way, hh, 0].astype(f32)

    def store(j):
        lanes = pl.ds(pl.multiple_of(j * slab, slab), slab)
        return pltpu.make_async_copy(made.at[:, lanes], result.at[:, lanes], bulk.at[4])

    def finish(j, halves=(None,)):
        for way in range(2):
            for h in halves:
                last_leg(j, way, h).wait_recv()
        for way in range(2):
            these = slice(way * part, (way + 1) * part)
            for hh, cols in columns(None):
                lanes = pl.ds(pl.multiple_of(j * slab + hh * thin, thin), thin)
                summed = ffn_own[j, these, cols] + last_in[j, way, hh].astype(f32)
                made[these, lanes] = (middle[these, lanes].astype(f32) + summed).astype(bf16)
        store(j).start()

    def slab_of(rank, turn):
        return order[rank] * SIDES + (x, 1 - x)[turn]

    def both(act, rank):
        for turn in range(SIDES):
            act(slab_of(rank, turn))

    def down_step(rank, when):
        for a in (3, 4):
            if rank == 1:
                line_step(a, 1, when=when)
                line_step(a, 2, when=when_all(when, inner))
            elif rank == 2:
                line_step(a, 2, when=when_all(when, outer))
            elif rank:
                line_step(a, rank, when=when)

    def down_core(rank, when):
        for a in (3, 4):
            arrive(theirs(a, order[rank]), core_recv.at[a, order[rank]], when)

    for rank in range(last):
        down_step(rank, straight)
        down_core(rank, crossed)
        lower(slab_of(rank, 0))
        down_step(rank, crossed)
        down_core(rank, straight)
        lower(slab_of(rank, 1))
        if rank:
            both(pass_on, rank - 1)
    both(finish, 0)
    soon, late = order[last] * SIDES + x, order[last] * SIDES + 1 - x
    for a in (3, 4):
        line_step(a, last, when=straight)
    for a in (3, 4):
        arrive(theirs(a, order[last]), core_recv.at[a, order[last]], crossed)
    with jax.named_scope("ldot"):
        lower(soon, split=True)
    for h in range(2):
        with jax.named_scope("lstep"):
            line_step(3 + h, last, when=crossed)
            arrive(theirs(3 + h, order[last]), core_recv.at[3 + h, order[last]], straight)
        with jax.named_scope("ldot"):
            lower(late, h)
    both(pass_on, last - 1)
    pass_on(soon, 0, (1,))
    pass_on(soon, 1, (1,))
    pass_on(late, 0, (0,))
    pass_on(late, 1, (0,))
    pass_on(soon, 0, (0,))
    pass_on(late, 0, (1,))
    for rank in range(1, last - 1):
        both(finish, rank)
    pass_on(late, 1, (1,))
    pass_on(soon, 1, (0,))
    both(finish, last - 1)
    for j in (soon, late):
        finish(j, (0, 1))

    for when, make in flights:
        if when is None:
            make().wait_send()
        else:
            pl.when(when)(lambda make=make: make().wait_send())

    @pl.when(crossed)
    def _():
        gone(mine(2, z), swap_send.at[0])
        gone(down_full.at[z * SIDES + x], swap_send.at[1])

    mine_out = pl.ds(pl.multiple_of(c * chans, chans), chans)
    gone(in_full.at[c, pl.ds(0, depth * slab), :], side_send.at[0])
    gone(out_full.at[pl.ds(0, depth), mine_out, :], side_send.at[1])
    gone(in_full.at[c], core_send.at[0])
    gone(out_full.at[:, mine_out, :], core_send.at[1])
    gone(up_full.at[pl.ds(0, depth)], core_send.at[2])
    for h in range(2):
        gone(down_full.at[pl.ds(0, depth), h], core_send.at[3 + h])
    gone(mix_send, bulk.at[0])
    gone(rows_two.at[pl.ds(0, 3 * rows), :], bulk.at[1])
    gone(pair_out, bulk.at[2])
    gone(last_out, bulk.at[3])
    pltpu.make_async_copy(made, result, bulk.at[4]).wait()


def resident(
    n_fs, n_tp, resid, mix_gain, in_weight, conv_taps, recur_gate_w, input_gate_w, decay_rate,
    out_weight, mlp_gain, up_gate_w, up_val_w, ffn_taps, down_weight,
):
    depth = n_fs // SIDES
    rows, width = resid.shape
    slab, chans = in_weight.shape
    units = up_gate_w.shape[1]
    slabs = width // slab
    tiles = units // LANES
    bf16, f32 = jnp.bfloat16, jnp.float32
    hbm = pl.BlockSpec(memory_space=pl.ANY)
    dma = pltpu.SemaphoreType.DMA
    return pl.pallas_call(
        functools.partial(resident_kernel, depth),
        out_shape=jax.ShapeDtypeStruct((rows, width), bf16),
        in_specs=[hbm] * 13,
        out_specs=hbm,
        scratch_shapes=[
            pltpu.VMEM((1, width), f32),
            pltpu.VMEM((1, width), f32),
            pltpu.VMEM(conv_taps.shape, f32),
            pltpu.VMEM((1, chans), f32),
            pltpu.VMEM(ffn_taps.shape, f32),
            pltpu.VMEM(recur_gate_w.shape, bf16),
            pltpu.VMEM(input_gate_w.shape, bf16),
            dma((7,)),
            pltpu.VMEM((rows, width), bf16),
            pltpu.VMEM((CORES, width, chans), bf16),
            pltpu.VMEM((slabs, CORES * chans, slab), bf16),
            pltpu.VMEM((slabs, tiles, slab, 2 * LANES), bf16),
            pltpu.VMEM((slabs, 2, units, slab // 2), bf16),
            pltpu.VMEM((CORES, 8, chans + units), f32),
            pltpu.VMEM((CORES, chans // LANES, LANES, 2 * LANES), bf16),
            pltpu.VMEM((2 * rows, width), bf16),
            pltpu.VMEM((2 * rows, CORES * chans), bf16),
            pltpu.VMEM((2 * rows, CORES * chans), bf16),
            pltpu.VMEM((slabs, rows, slab), f32),
            pltpu.VMEM((slabs, rows, slab), bf16),
            pltpu.VMEM((slabs, rows, slab), bf16),
            pltpu.VMEM((rows, width), bf16),
            pltpu.VMEM((4 * rows, width), bf16),
            pltpu.VMEM((4 * rows, units), bf16),
            pltpu.VMEM((tiles, 4 * rows, 2 * LANES), bf16),
            pltpu.VMEM((slabs, 2, rows // 2, slab), f32),
            pltpu.VMEM((slabs, 2, 2, 2, rows // 2, slab // 2), bf16),
            pltpu.VMEM((slabs, 2, 2, 2, rows // 2, slab // 2), bf16),
            pltpu.VMEM((slabs, 2, 2, rows // 2, slab // 2), bf16),
            pltpu.VMEM((slabs, 2, 2, rows // 2, slab // 2), bf16),
            pltpu.VMEM((rows, width), bf16),
            dma((6,)),
            dma((5, depth)), dma((5,)), dma((5, depth)),
            dma((2,)), dma((2, depth)),
            dma((5,)), dma((5, depth)),
            dma((2,)), dma((2,)),
            dma((2,)), dma((2,)),
            dma((2,)),
            dma((slabs,)),
            dma((2, 3)),
            dma((slabs, 2)), dma((2, 2)),
            dma((slabs, 2)), dma((2, 2)),
            dma((5,)),
            dma((2,)), dma((2,)), dma((2,)),
        ],
        compiler_params=pltpu.CompilerParams(
            collective_id=0, has_side_effects=True, vmem_limit_bytes=VMEM_BYTES
        ),
    )(
        resid, mix_gain.reshape(1, -1), mlp_gain.reshape(1, -1), conv_taps, decay_rate.reshape(1, -1),
        ffn_taps, recur_gate_w, input_gate_w, in_weight, out_weight, up_gate_w, up_val_w, down_weight,
    )


def solution(mesh):
    in_specs = (
        P(("fs", "tp"), None),
        P(),
        P("fs", "tp"),
        P(None, "tp"),
        P("tp", None, None),
        P("tp", None, None),
        P("tp"),
        P("tp", "fs"),
        P(),
        P("fs", "tp"),
        P("fs", "tp"),
        P(None, "tp"),
        P("tp", "fs"),
    )
    out_specs = P(("fs", "tp"), None)
    n_fs, n_tp = mesh.shape["fs"], mesh.shape["tp"]
    body = functools.partial(resident if fits(n_fs, n_tp) else shards, n_fs, n_tp)
    return jax.shard_map(body, mesh=mesh, in_specs=in_specs, out_specs=out_specs, check_vma=False)
```

```python
import functools

import jax
import jax.numpy as jnp
from jax import lax
from jax.experimental import pallas as pl
from jax.experimental.pallas import tpu as pltpu
from jax.sharding import PartitionSpec as P

GATE_BLOCK = 64
SEQ_LEN = 128
LANES = 128
CORES = 2


def rms_scale(rows_in, gain_vec):
    wide = rows_in.astype(jnp.float32)
    return wide * lax.rsqrt(jnp.mean(wide * wide, axis=-1, keepdims=True) + 1e-06) * gain_vec


def causal_taps(values, tap_weights):
    width = tap_weights.shape[0]
    length = values.shape[1]
    padded = jnp.pad(values, ((0, 0), (width - 1, 0), (0, 0)))
    summed = jnp.zeros_like(values)
    for tap_index in range(width):
        summed = summed + padded[:, tap_index : tap_index + length] * tap_weights[tap_index]
    return summed


def negative_expm1(arg):
    series = jnp.ones_like(arg)
    for order in range(8, 1, -1):
        series = 1.0 + arg * (1.0 / order) * series
    return jnp.where(arg > -0.5, -arg * series, 1.0 - jnp.exp(arg))


def shift_rows(values, distance, rows, fill):
    return jnp.where(rows >= distance, pltpu.roll(values, distance, 0), fill)


def recurrence_kernel(projected_ref, taps_ref, gates_ref, rate_ref, out_ref):
    width = taps_ref.shape[0]
    rows = lax.broadcasted_iota(jnp.int32, (SEQ_LEN, LANES), 0)
    for chunk in range(projected_ref.shape[1] // LANES):
        cols = slice(chunk * LANES, (chunk + 1) * LANES)
        values = projected_ref[:, cols].astype(jnp.float32)
        conv = values * taps_ref[width - 1 : width, cols]
        for back in range(1, width):
            tap = taps_ref[width - 1 - back : width - back, cols]
            conv = conv + shift_rows(values, back, rows, 0.0) * tap
        gates = jax.nn.sigmoid(
            jnp.dot(
                conv.astype(jnp.bfloat16), gates_ref[chunk], preferred_element_type=jnp.float32
            )
        )
        rgate = gates[:, :LANES]
        igate = gates[:, LANES:]
        logdecay = -8.0 * rgate * rate_ref[:, cols]
        decay = jnp.exp(logdecay)
        state = jnp.sqrt(negative_expm1(2.0 * logdecay)) * (igate * conv)
        distance = 1
        while distance < SEQ_LEN:
            state = state + decay * shift_rows(state, distance, rows, 0.0)
            if 2 * distance < SEQ_LEN:
                decay = decay * shift_rows(decay, distance, rows, 1.0)
            distance *= 2
        out_ref[:, cols] = state.astype(jnp.bfloat16)


def pair_blocks(blocks):
    pairs = blocks.reshape(-1, 2, GATE_BLOCK, GATE_BLOCK)
    blank = jnp.zeros_like(pairs[:, 0])
    upper = jnp.concatenate([pairs[:, 0], blank], axis=2)
    lower = jnp.concatenate([blank, pairs[:, 1]], axis=2)
    return jnp.concatenate([upper, lower], axis=1)


def recurrence(projected, conv_taps, gates, decay_rate):
    count, channels = projected.shape
    whole = lambda shape: pl.BlockSpec(shape, lambda seq: (0,) * len(shape))
    return pl.pallas_call(
        recurrence_kernel,
        grid=(count // SEQ_LEN,),
        in_specs=[
            pl.BlockSpec((SEQ_LEN, channels), lambda seq: (seq, 0)),
            whole(conv_taps.shape),
            whole(gates.shape),
            whole((1, channels)),
        ],
        out_specs=pl.BlockSpec((SEQ_LEN, channels), lambda seq: (seq, 0)),
        out_shape=jax.ShapeDtypeStruct(projected.shape, jnp.bfloat16),
        cost_estimate=pl.CostEstimate(
            flops=count * channels * 600, bytes_accessed=count * channels * 4,
            transcendentals=count * channels * 6,
        ),
    )(projected, conv_taps, gates, decay_rate.reshape(1, channels))


def gather_groups(block, n_tp):
    sides = n_tp // CORES
    swap = [(i, i ^ 1) for i in range(n_tp)]
    groups = []
    for distance in range(sides):
        mine = block
        if distance:
            back = [
                (i, ((i // CORES - distance) % sides) * CORES + i % CORES) for i in range(n_tp)
            ]
            mine = lax.ppermute(block, "tp", back)
        groups.append(jnp.concatenate([mine, lax.ppermute(mine, "tp", swap)], axis=0))
    return groups


def scatter_sum(partial_of, n_tp):
    sides = n_tp // CORES
    swap = [(i, i ^ 1) for i in range(n_tp)]
    total = 0.0
    for distance in reversed(range(sides)):
        partial = partial_of(distance)
        half = partial.shape[0] // 2
        other = lax.ppermute(partial[half:], "tp", swap)
        pair = partial[:half].astype(jnp.float32) + other.astype(jnp.float32)
        if distance:
            ahead = [
                (i, ((i // CORES + distance) % sides) * CORES + i % CORES) for i in range(n_tp)
            ]
            pair = lax.ppermute(pair.astype(jnp.bfloat16), "tp", ahead).astype(jnp.float32)
        total = total + pair
    return total


def gather_weight(block, n_fs, n_tp):
    inner = n_tp // CORES if n_fs % (n_tp // CORES) == 0 else 1
    outer = n_fs // inner
    me = lax.axis_index("fs")
    parts = [block]
    for distance in range(1, outer):
        back = [(i, (i - distance * inner) % n_fs) for i in range(n_fs)]
        parts.append(lax.ppermute(block, "fs", back))
    start = lax.rem(outer - me // inner, outer)
    column = lax.dynamic_slice_in_dim(jnp.stack(parts + parts[:-1]), start, outer, 0)
    parts = [column]
    for distance in range(1, inner):
        back = [(i, i // inner * inner + (i - distance) % inner) for i in range(n_fs)]
        parts.append(lax.ppermute(column, "fs", back))
    start = lax.rem(inner - lax.rem(me, inner), inner)
    stacked = jnp.stack(parts + parts[:-1], axis=1)
    stacked = lax.dynamic_slice_in_dim(stacked, start, inner, 1)
    return stacked.reshape((n_fs,) + block.shape)


def side_by_side(stacked):
    return jnp.transpose(stacked, (1, 0, 2)).reshape(stacked.shape[1], -1)


def dot(left, right):
    return jnp.dot(left, right, preferred_element_type=jnp.float32).astype(jnp.bfloat16)


def shards(
    n_fs,
    n_tp,
    resid,
    mix_gain,
    in_weight,
    conv_taps,
    recur_gate_w,
    input_gate_w,
    decay_rate,
    out_weight,
    mlp_gain,
    up_gate_w,
    up_val_w,
    ffn_taps,
    down_weight,
):
    gate_full = lax.all_gather(up_gate_w, "fs", axis=0, tiled=True)
    val_full = lax.all_gather(up_val_w, "fs", axis=0, tiled=True)
    cut = down_weight.shape[0] - down_weight.shape[0] // (2 * LANES) * LANES
    down_head = lax.all_gather(down_weight[:cut], "fs", axis=1, tiled=True)
    in_full = gather_weight(in_weight, n_fs, n_tp).reshape(-1, in_weight.shape[1])
    out_full = side_by_side(gather_weight(out_weight, n_fs, n_tp))
    later = lax.optimization_barrier((down_weight[cut:], in_full))[0]
    down_tail = side_by_side(gather_weight(later, n_fs, n_tp))
    gates = jnp.concatenate([pair_blocks(recur_gate_w), pair_blocks(input_gate_w)], axis=2)

    normed = rms_scale(resid, mix_gain).astype(jnp.bfloat16)
    recurred = [
        recurrence(dot(rows, in_full), conv_taps, gates, decay_rate)
        for rows in gather_groups(normed, n_tp)
    ]
    mixed_sum = scatter_sum(lambda distance: dot(recurred[distance], out_full), n_tp)
    middle = (resid.astype(jnp.float32) + mixed_sum).astype(jnp.bfloat16)
    normed_two = rms_scale(middle, mlp_gain).astype(jnp.bfloat16)

    hidden = []
    for rows in gather_groups(normed_two, n_tp):
        gate_pre = dot(rows, gate_full)
        value_pre = dot(rows, val_full)
        seqs = gate_pre.shape[0] // SEQ_LEN
        gate_conv = causal_taps(
            gate_pre.astype(jnp.float32).reshape(seqs, SEQ_LEN, -1), ffn_taps
        ).reshape(gate_pre.shape)
        hidden.append((jax.nn.silu(gate_conv) * value_pre.astype(jnp.float32)).astype(jnp.bfloat16))
    tails = [
        jnp.dot(rows[:, cut:], down_tail, preferred_element_type=jnp.float32) for rows in hidden
    ]

    def down_partial(distance):
        head = jnp.dot(hidden[distance][:, :cut], down_head, preferred_element_type=jnp.float32)
        return (head + tails[distance]).astype(jnp.bfloat16)

    ffn_sum = scatter_sum(down_partial, n_tp)
    return (middle.astype(jnp.float32) + ffn_sum).astype(jnp.bfloat16)


MESH = pl.DeviceIdType.MESH
SIDES = 2
VMEM_BYTES = 66_000_000


def fits(n_fs, n_tp):
    return n_tp == SIDES * CORES and n_fs == SIDES * 2 * SIDES


def line_order(depth, z):
    ranks = []
    for here in range(depth):
        up_first = here < depth / 2
        others = [p for p in range(depth) if p != here]
        others.sort(key=lambda p: (abs(p - here), (p < here) == up_first))
        ranks.append([here] + others)
    order = []
    for rank in range(depth):
        place = jnp.int32(0)
        for here in range(depth):
            place = jnp.where(z == here, ranks[here][rank], place)
        order.append(place)
    return order


def resident_kernel(
    depth,
    resid_in, gain_one_in, gain_two_in, conv_taps_in, decay_rate_in, ffn_taps_in, recur_gate_in, input_gate_in,
    in_w, out_w, gate_w, val_w, down_w,
    result,
    gain_one, gain_two, conv_taps, decay_rate, ffn_taps, recur_gate, input_gate, table_sem,
    resid, in_full, out_full, up_full, down_full, param_full, gate_full,
    normed, proj, recurred, mix_own, mix_send, mix_recv, middle, rows_two, hidden,
    sums, ffn_next, pair_out, pair_in, last_out, last_in, made,
    local_sem, line_send, line_twin, line_recv, side_send, side_recv, core_send, core_recv,
    swap_send, swap_recv, small_send, small_recv, row_sems, mix_recv_sem, ag_recv,
    pair_sem, pair_half, last_sem, last_half, bulk, far_send, far_recv, far_core,
):
    f32, bf16 = jnp.float32, jnp.bfloat16
    fs, tp = lax.axis_index("fs"), lax.axis_index("tp")
    z, x = fs // SIDES, lax.rem(fs, SIDES)
    y, c = tp // CORES, lax.rem(tp, CORES)
    rows, width = resid.shape
    slab, chans = in_w.shape
    taps, ffn_width = conv_taps.shape[0], ffn_taps.shape[0]
    tiles = gate_w.shape[1] // LANES
    slabs = width // slab
    n_seq = rows // SEQ_LEN
    order = line_order(depth, z)
    straight, crossed = x == c, x != c
    has_up, has_down = z < depth - 1, z > 0
    inner = jnp.logical_and(has_up, has_down)
    outer = jnp.logical_not(inner)
    near, far = range(1, min(3, depth)), range(3, depth)

    at = lambda zz, xx, yy, cc: (zz * SIDES + xx, yy * CORES + cc)
    up, down = at(z + 1, x, y, c), at(z - 1, x, y, c)
    side, core, swap = at(z, 1 - x, y, c), at(z, x, y, 1 - c), at(z, c, y, x)
    across = at(z, x, 1 - y, c)

    barrier = pltpu.get_barrier_semaphore()
    greet = lambda dev: pl.semaphore_signal(barrier, inc=1, device_id=dev, device_id_type=MESH)
    for dev in (side, core, across):
        greet(dev)
    for when, dev in ((has_up, up), (has_down, down), (crossed, swap)):
        pl.when(when)(functools.partial(greet, dev))
    one = lambda when: when.astype(jnp.int32)
    pl.semaphore_wait(barrier, 3 + one(has_up) + one(has_down) + one(crossed))

    flights = []

    def when_all(*conds):
        conds = [cond for cond in conds if cond is not None]
        return functools.reduce(jnp.logical_and, conds) if conds else None

    def remote(src, dst, ss, rs, dev):
        return pltpu.make_async_remote_copy(
            src_ref=src, dst_ref=dst, send_sem=ss, recv_sem=rs, device_id=dev, device_id_type=MESH
        )

    def send(src, dst, ss, rs, dev, when=None, alone=True):
        make = functools.partial(remote, src, dst, ss, rs, dev)
        if when is None:
            make().start()
        else:
            pl.when(when)(lambda: make().start())
        if alone:
            flights.append((when, make))

    def gone(whole, ss):
        remote(whole, whole, ss, ss, core).wait_send()

    def arrive(dst, rs, when=None):
        wait = lambda: remote(dst, dst, rs, rs, core).wait_recv()
        if when is None:
            wait()
        else:
            pl.when(when)(wait)

    def row_slab(zz, xx):
        return pl.ds(pl.multiple_of((zz * SIDES + xx) * slab, slab), slab)

    def place(a, zz, xx, cc):
        if a == 0:
            return in_full.at[cc, row_slab(zz, xx), :]
        if a == 1:
            return out_full.at[zz * SIDES + xx, pl.ds(pl.multiple_of(cc * chans, chans), chans), :]
        if a == 2:
            return up_full.at[zz * SIDES + xx]
        return down_full.at[zz * SIDES + xx, a - 3]

    def mine(a, zz):
        return place(a, zz, x, c) if a < 2 else place(a, zz, c, c)

    def theirs(a, zz):
        return place(a, zz, x, 1 - c) if a < 2 else place(a, zz, 1 - c, c)

    def along(a, zz, src=None, when=None, own=False):
        dst = mine(a, zz)
        src = dst if src is None else src
        ups = has_up if own else jnp.logical_and(zz < z, has_up)
        downs = has_down if own else jnp.logical_and(zz > z, has_down)
        twin = line_twin.at[a] if own else line_send.at[a, zz]
        send(src, dst, line_send.at[a, zz], line_recv.at[a, zz], up, when_all(ups, when))
        send(src, dst, twin, line_recv.at[a, zz], down, when_all(downs, when))

    def to_side(a, zz, src=None, when=None):
        dst = mine(a, zz)
        send(dst if src is None else src, dst, side_send.at[a], side_recv.at[a, zz], side, when, False)

    def core_sem(a, zz):
        return core_recv.at[a, 0] if a == 0 else core_recv.at[a, zz]

    def to_core(a, zz, src=None, when=None):
        dst = mine(a, zz)
        send(dst if src is None else src, dst, core_send.at[a], core_sem(a, zz), core, when, False)

    def line_step(a, rank, when=None):
        if rank >= depth:
            return
        zz = order[rank]
        arrive(mine(a, zz), line_recv.at[a, zz], when)
        along(a, zz, when=when)
        if a < 2:
            to_side(a, zz, when=when_all(when, (None, crossed)[a]))
        to_core(a, zz, when=when)

    def side_step(a, rank):
        if rank >= depth:
            return
        zz = order[rank]
        dst = place(a, zz, 1 - x, c)
        arrive(dst, side_recv.at[a, zz])
        send(dst, dst, core_send.at[a], core_sem(a, zz), core, None, False)

    in_copy = pltpu.make_async_copy(in_w, mine(0, z), local_sem.at[0])
    out_copy = pltpu.make_async_copy(out_w, mine(1, z), local_sem.at[1])
    up_copy = pltpu.make_async_copy(mine(2, z), mine(2, z), local_sem.at[2])
    thin = slab // 2
    down_part = lambda h: down_w.at[:, pl.ds(h * thin, thin)]
    down_copies = [pltpu.make_async_copy(down_part(h), mine(3 + h, z), local_sem.at[3 + h]) for h in range(2)]
    resid_copy = pltpu.make_async_copy(resid_in, resid, local_sem.at[5])

    def up_parts():
        for tile in range(tiles):
            for half, weight in enumerate((gate_w, val_w)):
                yield (
                    weight.at[:, pl.ds(tile * LANES, LANES)],
                    up_full.at[z * SIDES + x, tile, :, pl.ds(half * LANES, LANES)],
                )

    resid_copy.start()
    along(0, z, src=in_w, own=True)
    to_side(0, z, src=in_w)
    to_core(0, z, src=in_w)
    in_copy.start()
    out_copy.start()

    table_copies = [
        pltpu.make_async_copy(src, dst, table_sem.at[i])
        for i, (src, dst) in enumerate(
            (
                (gain_one_in, gain_one), (gain_two_in, gain_two), (conv_taps_in, conv_taps),
                (decay_rate_in, decay_rate), (ffn_taps_in, ffn_taps), (recur_gate_in, recur_gate),
                (input_gate_in, input_gate),
            )
        )
    ]
    for copy in table_copies:
        copy.start()
    for copy in table_copies:
        copy.wait()
    param_full[c, 0:taps, 0:chans] = conv_taps[...]
    param_full[c, taps : taps + 1, 0:chans] = decay_rate[...]
    param_full[c, 0:ffn_width, chans:] = ffn_taps[...]
    spot = lambda axis: lax.broadcasted_iota(jnp.int32, (GATE_BLOCK, LANES), axis)
    for half in range(LANES // GATE_BLOCK):
        spread = (spot(0) + half * GATE_BLOCK == spot(1)).astype(f32).astype(bf16)
        for kind, blocks in enumerate((recur_gate, input_gate)):
            for pair in range(chans // LANES):
                gate_full[
                    c, pair, half * GATE_BLOCK : (half + 1) * GATE_BLOCK, kind * LANES : (kind + 1) * LANES
                ] = jnp.dot(blocks[2 * pair + half], spread, preferred_element_type=f32).astype(bf16)
    resid_copy.wait()
    wide = resid[...].astype(f32)
    scale = lax.rsqrt(jnp.mean(wide * wide, axis=-1, keepdims=True) + 1e-06)
    normed[0:rows, :] = (wide * scale * gain_one[...]).astype(bf16)
    for i, full in enumerate((param_full, gate_full)):
        send(full.at[c], full.at[c], small_send.at[i], small_recv.at[i], core)
    send(normed.at[pl.ds(0, rows), :], normed.at[pl.ds(rows, rows), :], row_sems.at[0], row_sems.at[1], across)

    @pl.when(straight)
    def _():
        for src, dst in up_parts():
            pltpu.make_async_copy(src, dst, local_sem.at[2]).start()
        for copy in down_copies:
            copy.start()

    for rank in near:
        line_step(0, rank)
    along(1, z, src=out_w, own=True)
    to_core(1, z, src=out_w)
    side_step(0, 0)
    side_step(0, 1)

    def swap_some(parts):
        @pl.when(crossed)
        def _():
            for src, dst in parts:
                remote(src, dst, swap_send.at[0], swap_recv.at[0], swap).start()

    parts = list(up_parts())
    swap_some(parts[:tiles])
    for rank in far:
        line_step(0, rank)
    swap_some(parts[tiles:])
    to_side(1, z, src=out_w, when=crossed)
    side_step(0, 2)
    for rank in near:
        line_step(1, rank)

    def out_and_up(when):
        for rank in far:
            line_step(1, rank, when=when)
        ready = jnp.logical_and(straight, when)

        @pl.when(ready)
        def _():
            up_copy.wait()
            for copy in down_copies:
                copy.wait()

        along(2, z, when=ready, own=True)
        to_core(2, z, when=ready)

    out_and_up(inner)
    for rank in far:
        side_step(0, rank)
    in_copy.wait()
    out_copy.wait()
    for i, full in enumerate((param_full, gate_full)):
        arrive(full.at[1 - c], small_recv.at[i])
    arrive(in_full.at[1 - c], core_recv.at[0, 0])
    arrive(normed.at[pl.ds(rows, rows), :], row_sems.at[1])

    wide_n = 2 * LANES
    per = chans // wide_n

    def project(i, _):
        cc, h = i // per, lax.rem(i, per)
        lanes = pl.ds(pl.multiple_of(h * wide_n, wide_n), wide_n)
        to = pl.ds(pl.multiple_of(i * wide_n, wide_n), wide_n)
        proj[:, to] = jnp.dot(normed[...], in_full[cc, :, lanes], preferred_element_type=f32).astype(bf16)
        return 0

    lax.fori_loop(0, CORES * per, project, 0)

    to_side(1, z, src=out_w, when=straight)
    for rank in near:
        to_side(1, order[rank], when=straight)
    out_and_up(outer)
    for rank in far:
        to_side(1, order[rank], when=straight)
    for h in range(2):
        send(down_part(h), place(3 + h, z, x, c), swap_send.at[1], swap_recv.at[1], swap, crossed, False)

    position = lax.broadcasted_iota(jnp.int32, (SEQ_LEN, LANES), 0)
    chan_tiles = chans // LANES

    def recur(seq):
        where = pl.ds(seq * SEQ_LEN, SEQ_LEN)

        def tile_step(i, _):
            cc, u = i // chan_tiles, lax.rem(i, chan_tiles)
            cols = pl.ds(pl.multiple_of(u * LANES, LANES), LANES)
            to = pl.ds(pl.multiple_of(i * LANES, LANES), LANES)
            values = proj[where, to].astype(f32)
            table = param_full[cc, 0 : taps + 1, cols]
            conv = values * table[taps - 1 : taps]
            for back in range(1, taps):
                conv = conv + shift_rows(values, back, position, 0.0) * table[taps - 1 - back : taps - back]
            both = jax.nn.sigmoid(jnp.dot(conv.astype(bf16), gate_full[cc, u], preferred_element_type=f32))
            logdecay = -8.0 * both[:, :LANES] * table[taps : taps + 1]
            decay = jnp.exp(logdecay)
            state = jnp.sqrt(negative_expm1(2.0 * logdecay)) * (both[:, LANES:] * conv)
            distance = 1
            while distance < SEQ_LEN:
                state = state + decay * shift_rows(state, distance, position, 0.0)
                if 2 * distance < SEQ_LEN:
                    decay = decay * shift_rows(decay, distance, position, 1.0)
                distance *= 2
            recurred[where, to] = state.astype(bf16)
            return 0

        lax.fori_loop(0, CORES * chan_tiles, tile_step, 0)

    for seq in reversed(range(2 * n_seq)):
        recur(seq)
        if seq < 2:
            side_step(1, 1 - seq)

    arrive(mine(2, z), swap_recv.at[0], crossed)
    along(2, z, when=crossed, own=True)
    to_core(2, z, when=crossed)

    def mix_copy(j):
        return remote(mix_send.at[j], mix_recv.at[j], bulk.at[0], mix_recv_sem.at[j], across)

    for rank in range(depth):
        zz = order[rank]
        if rank >= 2:
            side_step(1, rank)
        theirs_out = pl.ds(pl.multiple_of((1 - c) * chans, chans), chans)
        arrive(out_full.at[pl.ds(zz * SIDES, SIDES), theirs_out, :], core_recv.at[1, zz])

        def mix(s, _):
            j = zz * SIDES + s
            both = jnp.dot(recurred[...], out_full[j], preferred_element_type=f32)
            mix_send[j] = both[rows:].astype(bf16)
            mix_copy(j).start()
            mix_own[j] = both[:rows]
            return 0

        lax.fori_loop(0, SIDES, mix, 0)
        if rank == 1:
            with jax.named_scope("up1_straight"):
                line_step(2, 1, when=straight)
                line_step(2, 2, when=when_all(straight, inner))

    total = jnp.zeros((rows, 1), f32)
    for j in range(slabs):
        mix_copy(j).wait_recv()
        lanes = slice(j * slab, (j + 1) * slab)
        value = (resid[:, lanes].astype(f32) + (mix_own[j] + mix_recv[j].astype(f32))).astype(bf16)
        middle[:, lanes] = value
        value = value.astype(f32)
        total = total + jnp.sum(value * value, axis=-1, keepdims=True)
    scale = lax.rsqrt(total * (1.0 / width) + 1e-06)
    rows_two[0:rows, :] = (middle[...].astype(f32) * scale * gain_two[...]).astype(bf16)

    part = rows // 2
    where = lambda slot, half: rows_two.at[pl.ds(slot * rows + half * part, part), :]
    send(where(0, 1), where(1, 1), bulk.at[1], ag_recv.at[0, 0], side, None, False)
    send(where(0, 0), where(2, 0), bulk.at[1], ag_recv.at[1, 0], across, None, False)
    send(where(0, 0), where(1, 0), bulk.at[1], ag_recv.at[0, 1], side, None, False)
    send(where(0, 1), where(2, 1), bulk.at[1], ag_recv.at[1, 1], across, None, False)
    line_step(2, 1, when=crossed)
    line_step(2, 2, when=when_all(crossed, inner))
    arrive(where(1, 1), ag_recv.at[0, 0])
    send(where(1, 1), where(3, 1), bulk.at[1], ag_recv.at[1, 2], across, None, False)
    arrive(where(2, 0), ag_recv.at[1, 0])
    send(where(2, 0), where(3, 0), bulk.at[1], ag_recv.at[0, 2], side, None, False)
    last = depth - 1
    cut_at = tiles // 2 + 1
    far_tiles = ((0, cut_at), (cut_at, tiles))
    far_piece = lambda ref, k: ref.at[pl.ds(far_tiles[k][0], far_tiles[k][1] - far_tiles[k][0])]
    zz = order[last]
    arrive(mine(2, zz), line_recv.at[2, zz], inner)
    for k in range(2):
        piece = far_piece(mine(2, zz), k)
        send(piece, piece, far_send.at[k], far_recv.at[k], up, when_all(inner, zz < z))
        send(piece, piece, far_send.at[k], far_recv.at[k], down, when_all(inner, zz > z))
    for k in range(2):
        piece = far_piece(mine(2, zz), k)
        send(piece, piece, core_send.at[2], far_core.at[k], core, inner, False)
    arrive(where(1, 0), ag_recv.at[0, 1])
    arrive(where(2, 1), ag_recv.at[1, 1])
    arrive(where(3, 0), ag_recv.at[0, 2])
    arrive(where(3, 1), ag_recv.at[1, 2])
    arrive(down_full.at[z * SIDES + c], swap_recv.at[1], crossed)
    for a in (3, 4):
        along(a, z, own=True)
        to_core(a, z)
    lift = 2 * rows
    reach = SIDES * slab
    for rank in range(2, last):
        line_step(2, rank, when=outer)
    for rank in range(last):
        arrive(theirs(2, order[rank]), core_recv.at[2, order[rank]])

    def product(t, here, rank):
        span = pl.ds(pl.multiple_of(order[rank] * reach, reach), reach)
        weight = up_full[pl.ds(order[rank] * SIDES, SIDES), t].reshape(reach, 2 * LANES)
        return jnp.dot(rows_two[here, span], weight, preferred_element_type=f32)

    def partial_tile(t, _):
        for block in range(2):
            here = slice(block * lift, (block + 1) * lift)
            pre = product(t, here, 0)
            for rank in range(1, last):
                pre = pre + product(t, here, rank)
            sums[t, here, :] = pre.astype(bf16)
        return 0

    lax.fori_loop(0, tiles, partial_tile, 0)
    row_in_seq = lax.rem(lax.broadcasted_iota(jnp.int32, (lift, LANES), 0), SEQ_LEN)

    def raise_tile(t, _):
        cols = pl.ds(pl.multiple_of(t * LANES, LANES), LANES)
        table = param_full[x, 0:ffn_width, pl.ds(pl.multiple_of(chans + t * LANES, LANES), LANES)]
        for block in range(2):
            here = slice(block * lift, (block + 1) * lift)
            pre = sums[t, here, :].astype(f32) + product(t, here, last)
            gate = pre[:, :LANES].astype(bf16).astype(f32)
            value = pre[:, LANES:].astype(bf16).astype(f32)
            conv = gate * table[ffn_width - 1 : ffn_width]
            for back in range(1, ffn_width):
                shifted = shift_rows(gate, back, row_in_seq, 0.0)
                conv = conv + shifted * table[ffn_width - 1 - back : ffn_width - back]
            hidden[here, cols] = (jax.nn.silu(conv) * value).astype(bf16)
        return 0

    for k in range(2):
        with jax.named_scope("up_last"):
            piece = far_piece(mine(2, order[last]), k)
            arrive(piece, far_recv.at[k], outer)
            send(piece, piece, core_send.at[2], far_core.at[k], core, outer, False)
            arrive(far_piece(theirs(2, order[last]), k), far_core.at[k])
        lax.fori_loop(*far_tiles[k], raise_tile, 0)

    ffn_own = mix_own

    def cut(ref, h):
        return ref if h is None else ref.at[h]

    def columns(h):
        return [(hh, slice(hh * thin, (hh + 1) * thin)) for hh in ((0, 1) if h is None else (h,))]

    def first_leg(j, way, h=None):
        sem = pair_half.at[j % SIDES, way] if h else pair_sem.at[j, way]
        return remote(cut(pair_out.at[j, way], h), cut(pair_in.at[j, way], h), bulk.at[2], sem, (side, across)[way])

    def last_leg(j, way, h=None):
        sem = last_half.at[j % SIDES, way] if h else last_sem.at[j, way]
        return remote(cut(last_out.at[j, way], h), cut(last_in.at[j, way], h), bulk.at[3], sem, (across, side)[way])

    def lower(j, h=None, split=False):
        cols = slice(None) if h is None else slice(h * thin, (h + 1) * thin)
        weight = jnp.concatenate([down_full[j, 0], down_full[j, 1]], axis=1) if h is None else down_full[j, h]
        block = jnp.dot(hidden[rows:, :], weight, preferred_element_type=f32)
        for way in range(2):
            for leg, slot in enumerate((way, 2)):
                first = slot * rows + way * part
                for hh, lanes in columns(h):
                    value = block[first : first + part, lanes if h is None else slice(None)]
                    pair_out[j, way, hh, leg] = value.astype(bf16)
        for part_h in (0, 1) if split else (h,):
            for way in range(2):
                first_leg(j, way, part_h).start()
        for way in range(2):
            first = (1 - way) * rows + way * part
            ffn_next[j, way, :, cols] = block[first : first + part]
        ffn_own[j, :, cols] = jnp.dot(hidden[:rows, :], weight, preferred_element_type=f32)

    def pass_on(j, h=None, ways=(0, 1)):
        for way in ways:
            these = slice(way * part, (way + 1) * part)
            first_leg(j, way, h).wait_recv()
            for hh, cols in columns(h):
                last_out[j, way, hh] = (
                    ffn_next[j, way, :, cols] + pair_in[j, way, hh, 1].astype(f32)
                ).astype(bf16)
            last_leg(j, way, h).start()
            for hh, cols in columns(h):
                ffn_own[j, these, cols] = ffn_own[j, these, cols] + pair_in[j, way, hh, 0].astype(f32)

    def store(j):
        lanes = pl.ds(pl.multiple_of(j * slab, slab), slab)
        return pltpu.make_async_copy(made.at[:, lanes], result.at[:, lanes], bulk.at[4])

    def finish(j, halves=(None,)):
        for way in range(2):
            for h in halves:
                last_leg(j, way, h).wait_recv()
        for way in range(2):
            these = slice(way * part, (way + 1) * part)
            for hh, cols in columns(None):
                lanes = pl.ds(pl.multiple_of(j * slab + hh * thin, thin), thin)
                summed = ffn_own[j, these, cols] + last_in[j, way, hh].astype(f32)
                made[these, lanes] = (middle[these, lanes].astype(f32) + summed).astype(bf16)
        store(j).start()

    def finish_half(j, h):
        lanes = pl.ds(pl.multiple_of(j * slab + h * thin, thin), thin)
        for way in range(2):
            these = slice(way * part, (way + 1) * part)
            last_leg(j, way, h).wait_recv()
            summed = ffn_own[j, these, h * thin : (h + 1) * thin] + last_in[j, way, h].astype(f32)
            made[these, lanes] = (middle[these, lanes].astype(f32) + summed).astype(bf16)
        pltpu.make_async_copy(made.at[:, lanes], result.at[:, lanes], bulk.at[4]).start()

    def slab_of(rank, turn):
        return order[rank] * SIDES + (x, 1 - x)[turn]

    def both(act, rank):
        for turn in range(SIDES):
            act(slab_of(rank, turn))

    def down_step(rank, when):
        for a in (3, 4):
            if rank == 1:
                line_step(a, 1, when=when)
                line_step(a, 2, when=when_all(when, inner))
            elif rank == 2:
                line_step(a, 2, when=when_all(when, outer))
            elif rank:
                line_step(a, rank, when=when)

    def down_core(rank, when):
        for a in (3, 4):
            arrive(theirs(a, order[rank]), core_recv.at[a, order[rank]], when)

    for rank in range(last):
        down_step(rank, straight)
        down_core(rank, crossed)
        lower(slab_of(rank, 0))
        down_step(rank, crossed)
        down_core(rank, straight)
        lower(slab_of(rank, 1))
        if rank:
            both(pass_on, rank - 1)
    both(finish, 0)
    soon, late = order[last] * SIDES + x, order[last] * SIDES + 1 - x
    for a in (3, 4):
        line_step(a, last, when=straight)
    for a in (3, 4):
        arrive(theirs(a, order[last]), core_recv.at[a, order[last]], crossed)
    with jax.named_scope("ldot"):
        lower(soon, split=True)
    for h in range(2):
        with jax.named_scope("lstep"):
            line_step(3 + h, last, when=crossed)
            arrive(theirs(3 + h, order[last]), core_recv.at[3 + h, order[last]], straight)
        with jax.named_scope("ldot"):
            lower(late, h)
    both(pass_on, last - 1)
    pass_on(soon, 0, (1,))
    pass_on(soon, 1, (1,))
    pass_on(late, 0, (0,))
    pass_on(late, 1, (0,))
    pass_on(soon, 0, (0,))
    pass_on(late, 0, (1,))
    for rank in range(1, last - 1):
        both(finish, rank)
    pass_on(late, 1, (1,))
    pass_on(soon, 1, (0,))
    both(finish, last - 1)
    for h in range(2):
        for j in (soon, late):
            finish_half(j, h)

    for when, make in flights:
        if when is None:
            make().wait_send()
        else:
            pl.when(when)(lambda make=make: make().wait_send())

    @pl.when(crossed)
    def _():
        gone(mine(2, z), swap_send.at[0])
        gone(down_full.at[z * SIDES + x], swap_send.at[1])

    mine_out = pl.ds(pl.multiple_of(c * chans, chans), chans)
    gone(in_full.at[c, pl.ds(0, depth * slab), :], side_send.at[0])
    gone(out_full.at[pl.ds(0, depth), mine_out, :], side_send.at[1])
    gone(in_full.at[c], core_send.at[0])
    gone(out_full.at[:, mine_out, :], core_send.at[1])
    gone(up_full.at[pl.ds(0, depth)], core_send.at[2])
    for h in range(2):
        gone(down_full.at[pl.ds(0, depth), h], core_send.at[3 + h])
    gone(mix_send, bulk.at[0])
    gone(rows_two.at[pl.ds(0, 3 * rows), :], bulk.at[1])
    gone(pair_out, bulk.at[2])
    gone(last_out, bulk.at[3])
    pltpu.make_async_copy(made, result, bulk.at[4]).wait()


def resident(
    n_fs, n_tp, resid, mix_gain, in_weight, conv_taps, recur_gate_w, input_gate_w, decay_rate,
    out_weight, mlp_gain, up_gate_w, up_val_w, ffn_taps, down_weight,
):
    depth = n_fs // SIDES
    rows, width = resid.shape
    slab, chans = in_weight.shape
    units = up_gate_w.shape[1]
    slabs = width // slab
    tiles = units // LANES
    bf16, f32 = jnp.bfloat16, jnp.float32
    hbm = pl.BlockSpec(memory_space=pl.ANY)
    dma = pltpu.SemaphoreType.DMA
    return pl.pallas_call(
        functools.partial(resident_kernel, depth),
        out_shape=jax.ShapeDtypeStruct((rows, width), bf16),
        in_specs=[hbm] * 13,
        out_specs=hbm,
        scratch_shapes=[
            pltpu.VMEM((1, width), f32),
            pltpu.VMEM((1, width), f32),
            pltpu.VMEM(conv_taps.shape, f32),
            pltpu.VMEM((1, chans), f32),
            pltpu.VMEM(ffn_taps.shape, f32),
            pltpu.VMEM(recur_gate_w.shape, bf16),
            pltpu.VMEM(input_gate_w.shape, bf16),
            dma((7,)),
            pltpu.VMEM((rows, width), bf16),
            pltpu.VMEM((CORES, width, chans), bf16),
            pltpu.VMEM((slabs, CORES * chans, slab), bf16),
            pltpu.VMEM((slabs, tiles, slab, 2 * LANES), bf16),
            pltpu.VMEM((slabs, 2, units, slab // 2), bf16),
            pltpu.VMEM((CORES, 8, chans + units), f32),
            pltpu.VMEM((CORES, chans // LANES, LANES, 2 * LANES), bf16),
            pltpu.VMEM((2 * rows, width), bf16),
            pltpu.VMEM((2 * rows, CORES * chans), bf16),
            pltpu.VMEM((2 * rows, CORES * chans), bf16),
            pltpu.VMEM((slabs, rows, slab), f32),
            pltpu.VMEM((slabs, rows, slab), bf16),
            pltpu.VMEM((slabs, rows, slab), bf16),
            pltpu.VMEM((rows, width), bf16),
            pltpu.VMEM((4 * rows, width), bf16),
            pltpu.VMEM((4 * rows, units), bf16),
            pltpu.VMEM((tiles, 4 * rows, 2 * LANES), bf16),
            pltpu.VMEM((slabs, 2, rows // 2, slab), f32),
            pltpu.VMEM((slabs, 2, 2, 2, rows // 2, slab // 2), bf16),
            pltpu.VMEM((slabs, 2, 2, 2, rows // 2, slab // 2), bf16),
            pltpu.VMEM((slabs, 2, 2, rows // 2, slab // 2), bf16),
            pltpu.VMEM((slabs, 2, 2, rows // 2, slab // 2), bf16),
            pltpu.VMEM((rows, width), bf16),
            dma((6,)),
            dma((5, depth)), dma((5,)), dma((5, depth)),
            dma((2,)), dma((2, depth)),
            dma((5,)), dma((5, depth)),
            dma((2,)), dma((2,)),
            dma((2,)), dma((2,)),
            dma((2,)),
            dma((slabs,)),
            dma((2, 3)),
            dma((slabs, 2)), dma((2, 2)),
            dma((slabs, 2)), dma((2, 2)),
            dma((5,)),
            dma((2,)), dma((2,)), dma((2,)),
        ],
        compiler_params=pltpu.CompilerParams(
            collective_id=0, has_side_effects=True, vmem_limit_bytes=VMEM_BYTES
        ),
    )(
        resid, mix_gain.reshape(1, -1), mlp_gain.reshape(1, -1), conv_taps, decay_rate.reshape(1, -1),
        ffn_taps, recur_gate_w, input_gate_w, in_weight, out_weight, up_gate_w, up_val_w, down_weight,
    )


def solution(mesh):
    in_specs = (
        P(("fs", "tp"), None),
        P(),
        P("fs", "tp"),
        P(None, "tp"),
        P("tp", None, None),
        P("tp", None, None),
        P("tp"),
        P("tp", "fs"),
        P(),
        P("fs", "tp"),
        P("fs", "tp"),
        P(None, "tp"),
        P("tp", "fs"),
    )
    out_specs = P(("fs", "tp"), None)
    n_fs, n_tp = mesh.shape["fs"], mesh.shape["tp"]
    body = functools.partial(resident if fits(n_fs, n_tp) else shards, n_fs, n_tp)
    return jax.shard_map(body, mesh=mesh, in_specs=in_specs, out_specs=out_specs, check_vma=False)
```
